32 devices in a mesh: ep: 4 (over z), tp: 8 (over y, x, core).
Axes of the slice: x: 2, y: 2, z: 4, core: 2. Of those that a mesh axis runs over, the one named last changes fastest.
Arguments:
- queries: bfloat16 [1024, 2048], P('ep', 'tp'), may hold values from -6 to 6
- key_rows: bfloat16 [1024, 1024], P('ep', 'tp'), may hold values from -6 to 6
- values: bfloat16 [1024, 1024], P('ep', 'tp'), may hold values from -140 to 140
- query_gain: float32 [64], replicated, may hold values from 0.55 to 7.5
- key_gain: float32 [64], replicated, may hold values from 0.55 to 7.5
- mix_gain: float32 [2048], replicated, may hold values from 0.1 to 1.9
- out_weight: bfloat16 [2048, 4096], P(None, 'tp'), may hold values from -0.125 to 0.125
- expert_input: bfloat16 [1024, 4096], P('ep', 'tp'), may hold values from -140 to 140
- expert_gain: float32 [4096], replicated, may hold values from 0.1 to 1.9
- route_ids: int32 [1024, 2], P('ep'), may hold values from 0 to 3, as said below
- route_weights: float32 [1024, 2], P('ep'), may hold values from 0.3 to 1.7
- expert_gate: bfloat16 [4, 4096, 2048], P('ep', None, 'tp'), may hold values from -0.09375 to 0.09375
- expert_up: bfloat16 [4, 4096, 2048], P('ep', None, 'tp'), may hold values from -0.09375 to 0.09375
- expert_down: bfloat16 [4, 2048, 4096], P('ep', None, 'tp'), may hold values from -0.125 to 0.125
Outputs:
- attended: bfloat16 [1024, 4096], P('ep', 'tp')
- expert_mix: bfloat16 [1024, 4096], P('ep', 'tp')
The draws below stay inside these ranges and needn't reach their ends.
Inputs may be any that keep to these rules, and one draw needn't show every extreme that they name: `route_ids`: the 2 experts of a row differ. In every aligned block of 256 rows no expert is named more than 171 times, and one expert, the same for all blocks, is named exactly 171 times in every block.
All inputs are finite; a program needn't handle non-finite values.
Results may differ from the reference program's by a relative error of at most 0.01.
The reference program's roundings to bfloat16 on the way count: a program that leaves them out, or rounds other values in their place, can miss the bound.
Values may be sent and summed in bfloat16 or wider, within the bound.
A program may use at most 64 MiB of HBM per device.

```python
import math
import jax
import jax.numpy as jnp
from jax import lax

D = 4096
Q_HEADS = 32
KV_HEADS = 16
HEAD = 64
FF = 2048
TOP_K = 2
GRID_W = 64
TOK_DEV = 256
TOKENS = 1024
EXPERTS = 4
CAP = 171
N_EP = 4


def draw_key_rows(key, part):
    field_data = jnp.clip(jax.random.normal(jax.random.fold_in(key, 7), (TOKENS, KV_HEADS * HEAD), jnp.float32), -6.0, 6.0)
    return field_data.astype(jnp.bfloat16)


def draw_queries(key, part):
    field_data = jnp.clip(jax.random.normal(jax.random.fold_in(key, 9), (TOKENS, Q_HEADS * HEAD), jnp.float32), -6.0, 6.0)
    return field_data.astype(jnp.bfloat16)


def rising_field(seed_key, row_count, column_count, group_width):
    pieces = jax.random.split(seed_key, 2)
    group_count = column_count // group_width
    position = (jnp.arange(column_count) // group_width).astype(jnp.float32) / max(group_count - 1, 1)
    jitter = jax.random.uniform(pieces[1], (column_count,), jnp.float32)
    log_scale = math.log(10.0) * 0.5 * (position + jitter)
    field_data = jnp.clip(jax.random.normal(pieces[0], (row_count, column_count), jnp.float32), -4.0, 4.0)
    return field_data * jnp.exp(log_scale)


def draw_values(key, part):
    return rising_field(jax.random.fold_in(key, 3), TOKENS, KV_HEADS * HEAD, HEAD).astype(jnp.bfloat16)


def draw_expert_input(key, part):
    return rising_field(jax.random.fold_in(key, 5), TOKENS, D, 1).astype(jnp.bfloat16)


def draw_query_gain(key, part):
    seed_key = jax.random.fold_in(key, 21)
    return jax.random.uniform(seed_key, (HEAD,), jnp.float32, 0.55, 1.45)


def draw_key_gain(key, part):
    seed_key = jax.random.fold_in(key, 23)
    return jax.random.uniform(seed_key, (HEAD,), jnp.float32, 0.55, 1.45)


def block_routes(seed_key, favored):
    ticket_total = TOK_DEV * TOP_K
    pieces = jax.random.split(seed_key, 3)
    ticket_order = jax.random.permutation(pieces[0], (EXPERTS - 1) * CAP)
    live_slots = (ticket_order < ticket_total - CAP).astype(jnp.int32).reshape(EXPERTS - 1, CAP)
    rest_counts = jnp.sum(live_slots, axis=1).astype(jnp.int32)
    everyone = jnp.arange(EXPERTS, dtype=jnp.int32)
    rest_index = jnp.clip(everyone - (everyone > favored).astype(jnp.int32), 0, max(EXPERTS - 2, 0))
    counts = jnp.where(everyone == favored, CAP, rest_counts[rest_index]).astype(jnp.int32)
    run_order = jax.random.permutation(pieces[1], EXPERTS).astype(jnp.int32)
    run_ends = jnp.cumsum(counts[run_order]).astype(jnp.int32)
    run_index = jnp.searchsorted(run_ends, jnp.arange(ticket_total, dtype=jnp.int32), side='right')
    tickets = run_order[run_index]
    by_row = tickets.reshape(TOP_K, TOK_DEV).T
    row_order = jax.random.permutation(pieces[2], TOK_DEV)
    return jnp.zeros((TOK_DEV, TOP_K), jnp.int32).at[row_order].set(by_row)


def draw_route_ids(key, part):
    base_key = jax.random.fold_in(key, 13)
    favored = jax.random.randint(jax.random.fold_in(base_key, 1), (), 0, EXPERTS).astype(jnp.int32)
    block_keys = jax.random.split(jax.random.fold_in(base_key, 2), N_EP)
    routes = jax.vmap(block_routes, in_axes=(0, None))(block_keys, favored)
    return routes.reshape(TOKENS, TOP_K).astype(jnp.int32)


def steps_of(key, extent, shards, least, high):
    def one(dim, parts):
        draws = jax.random.uniform(jax.random.fold_in(jax.random.fold_in(key, 6), dim), (parts,), jnp.float32, least / len(shards), high / len(shards))
        return jnp.repeat(jnp.exp(draws), extent[dim] // parts).reshape((-1,) + (1,) * (len(extent) - dim - 1))

    gain = one(*shards[0])
    for cut in shards[1:]:
        gain = gain * one(*cut)
    return gain


def scatter_about(own_key, dims, spread, limit, cuts=(), held_as=jnp.bfloat16):
    loudness = steps_of(own_key, dims, cuts, -0.22, 0.18) if cuts else 1.0
    result = jax.random.normal(own_key, dims, jnp.float32) * spread * loudness
    return jnp.minimum(jnp.maximum(result, -limit), limit).astype(held_as)


def setup_inputs(seed: int = 0) -> dict:
    key_of = jax.random.split(jax.random.key(seed), 15)
    queries = draw_queries(jax.random.fold_in(key_of[14], 71), 0)
    key_rows = draw_key_rows(jax.random.fold_in(key_of[14], 71), 0)
    values = draw_values(jax.random.fold_in(key_of[14], 71), 0)
    query_gain = draw_query_gain(jax.random.fold_in(key_of[14], 71), 0)
    key_gain = draw_key_gain(jax.random.fold_in(key_of[14], 71), 0)
    mix_gain = jnp.clip(1.0 + 0.18 * jax.random.normal(key_of[5], (Q_HEADS * HEAD,), jnp.float32), 0.1, 1.9)
    out_weight = scatter_about(key_of[6], (Q_HEADS * HEAD, D), (Q_HEADS * HEAD) ** -0.5, 0.125, ((1, 8),))
    expert_input = draw_expert_input(jax.random.fold_in(key_of[14], 71), 0)
    expert_gain = jnp.clip(1.0 + 0.18 * jax.random.normal(key_of[8], (D,), jnp.float32), 0.1, 1.9)
    route_ids = draw_route_ids(jax.random.fold_in(key_of[14], 71), 0)
    route_weights = jnp.clip(0.3 + 1.40000004 * jax.random.uniform(key_of[10], (TOKENS, TOP_K), jnp.float32) ** steps_of(key_of[10], (TOKENS, TOP_K), ((0, 4),), -0.2, 0.2), 0.3, 1.7)
    expert_gate = scatter_about(key_of[11], (EXPERTS, D, FF), D ** -0.5, 0.09375, ((0, 4), (2, 8)))
    expert_up = scatter_about(key_of[12], (EXPERTS, D, FF), D ** -0.5, 0.09375, ((0, 4), (2, 8)))
    expert_down = scatter_about(key_of[13], (EXPERTS, FF, D), FF ** -0.5, 0.125, ((0, 4), (2, 8)))
    return dict(queries=queries, key_rows=key_rows, values=values, query_gain=query_gain, key_gain=key_gain, mix_gain=mix_gain, out_weight=out_weight, expert_input=expert_input, expert_gain=expert_gain, route_ids=route_ids, route_weights=route_weights, expert_gate=expert_gate, expert_up=expert_up, expert_down=expert_down)


EPS = 1e-06
THETA = 10000.0

def turn_tables(length):
    half_width = HEAD // 2
    inverse = THETA ** (-jnp.arange(0, half_width, 2, dtype=jnp.float32) / half_width)
    positions = jnp.arange(length, dtype=jnp.int32)
    grid_rows = (positions // GRID_W).astype(jnp.float32)
    grid_cols = (positions % GRID_W).astype(jnp.float32)
    angles = jnp.concatenate([grid_rows[:, None] * inverse, grid_cols[:, None] * inverse], axis=-1)
    return (jnp.cos(angles), jnp.sin(angles))

def norm_turn(source, scale_gain, cosine_table, sine_table):
    length = source.shape[0]
    head_rows = source.astype(jnp.float32).reshape(length, -1, HEAD)
    head_rows = head_rows * lax.rsqrt(lax.optimization_barrier(jnp.mean(head_rows * head_rows, axis=-1, keepdims=True)) + EPS) * scale_gain
    pair_view = head_rows.reshape(length, head_rows.shape[1], HEAD // 2, 2)
    even_part = pair_view[..., 0]
    odd_part = pair_view[..., 1]
    cosine_part = cosine_table[:, None, :]
    sine_part = sine_table[:, None, :]
    turned = jnp.stack([even_part * cosine_part - odd_part * sine_part, even_part * sine_part + odd_part * cosine_part], axis=-1)
    return turned.reshape(length, -1).astype(jnp.bfloat16)

def attend_head(operands):
    query_group, key_head, value_head = operands
    length = query_group.shape[0]
    block_rows = math.gcd(length, 512)
    query_blocks = query_group.reshape(length // block_rows, block_rows, query_group.shape[1], HEAD)
    keys_float = key_head.astype(jnp.float32)
    values_float = value_head.astype(jnp.float32)

    def one_block(query_block):
        scores = jnp.einsum('rgd,nd->grn', query_block.astype(jnp.float32), keys_float) / math.sqrt(HEAD)
        row_max = lax.optimization_barrier(jnp.max(scores, axis=-1, keepdims=True))
        raw_weights = jnp.exp(scores - row_max)
        row_total = lax.optimization_barrier(jnp.sum(raw_weights, axis=-1))
        rounded = lax.optimization_barrier(raw_weights.astype(jnp.bfloat16)).astype(jnp.float32)
        summed = jnp.einsum('grn,nd->rgd', rounded, values_float)
        return (summed / jnp.transpose(row_total)[:, :, None]).astype(jnp.bfloat16)
    return lax.map(one_block, query_blocks).reshape(length, -1)

def reference(queries, key_rows, values, query_gain, key_gain, mix_gain, out_weight, expert_input, expert_gain, route_ids, route_weights, expert_gate, expert_up, expert_down):
    length = queries.shape[0]
    cosine_table, sine_table = turn_tables(length)
    query_turned = norm_turn(queries, query_gain, cosine_table, sine_table)
    key_turned = norm_turn(key_rows, key_gain, cosine_table, sine_table)
    group_size = Q_HEADS // KV_HEADS
    query_heads = query_turned.reshape(length, KV_HEADS, group_size, HEAD).transpose(1, 0, 2, 3)
    key_heads = key_turned.reshape(length, KV_HEADS, HEAD).transpose(1, 0, 2)
    value_heads = values.reshape(length, KV_HEADS, HEAD).transpose(1, 0, 2)
    heads_out = lax.map(attend_head, (query_heads, key_heads, value_heads))
    heads_out = heads_out.transpose(1, 0, 2).reshape(length, Q_HEADS * HEAD)
    heads_float = heads_out.astype(jnp.float32)
    mix_scale = lax.rsqrt(lax.optimization_barrier(jnp.mean(heads_float * heads_float, axis=-1)) + EPS)
    mix_in = (heads_float * mix_gain).astype(jnp.bfloat16)
    attended = (jnp.dot(mix_in, out_weight, preferred_element_type=jnp.float32) * mix_scale[:, None]).astype(jnp.bfloat16)
    blocks = N_EP
    copies = TOK_DEV * TOP_K
    ids_block = route_ids.reshape(blocks, copies).astype(jnp.int32)
    hit_marks = (ids_block[:, :, None] == jnp.arange(EXPERTS, dtype=jnp.int32)[None, None, :]).astype(jnp.int32)
    earlier = (jnp.cumsum(hit_marks, axis=1) - hit_marks).astype(jnp.int32)
    places = lax.optimization_barrier(jnp.sum(earlier * hit_marks, axis=2)).astype(jnp.int32)
    block_index = jnp.broadcast_to(jnp.arange(blocks, dtype=jnp.int32)[:, None], (blocks, copies))
    token_index = block_index * TOK_DEV + (jnp.arange(copies, dtype=jnp.int32) // TOP_K)[None, :]
    slot_table = jnp.full((EXPERTS, blocks, CAP), length, jnp.int32)
    slot_table = slot_table.at[ids_block, block_index, places].set(token_index.astype(jnp.int32))
    input_float = expert_input.astype(jnp.float32)
    expert_stat = lax.rsqrt(lax.optimization_barrier(jnp.mean(input_float * input_float, axis=-1)) + EPS)
    expert_scaled = (input_float * expert_gain).astype(jnp.bfloat16)
    scaled_pad = jnp.concatenate([expert_scaled, jnp.zeros((1, D), jnp.bfloat16)], axis=0)
    stat_pad = jnp.concatenate([expert_stat, jnp.zeros((1,), jnp.float32)], axis=0)

    def run_expert(operands):
        slot_tokens, gate_weight, up_weight, down_weight = operands
        flat_tokens = slot_tokens.reshape(-1)
        slot_input = scaled_pad[flat_tokens]
        row_stat = stat_pad[flat_tokens][:, None]
        gate_value = jnp.dot(slot_input, gate_weight, preferred_element_type=jnp.float32) * row_stat
        up_value = jnp.dot(slot_input, up_weight, preferred_element_type=jnp.float32) * row_stat
        hidden = (jax.nn.silu(gate_value) * up_value).astype(jnp.bfloat16)
        return jnp.dot(hidden, down_weight, preferred_element_type=jnp.float32).astype(jnp.bfloat16)
    outputs = lax.map(run_expert, (slot_table, expert_gate, expert_up, expert_down))
    picked = outputs[ids_block, block_index * CAP + places].astype(jnp.float32)
    weighted = picked * route_weights.reshape(blocks, copies)[:, :, None]
    expert_mix = lax.optimization_barrier(jnp.sum(weighted.reshape(length, TOP_K, D), axis=1)).astype(jnp.bfloat16)
    return (attended, expert_mix)
```

```python
import functools
import math

import jax
import jax.numpy as jnp
import numpy as np
from jax import lax
from jax.experimental import pallas as pl
from jax.experimental.pallas import tpu as pltpu
from jax.sharding import PartitionSpec as P

Q_HEADS = 32
KV_HEADS = 16
HEAD = 64
GRID_W = 64
EPS = 1e-06
THETA = 10000.0
MESH = pl.DeviceIdType.MESH
F32 = jnp.float32
BF16 = jnp.bfloat16


def gather_plan(n_tp):
    if n_tp == 8:
        return (
            (2, 0, None, None),
            (4, 0, None, None),
            (1, 0, None, None),
            (4, 2, 0, 0),
            (2, 4, 1, 1),
            (1, 2, None, 0),
            (1, 4, None, 1),
            (1, 6, 0, 3),
            (1, 6, 1, 4),
        )
    return tuple((m, 0, None, None) for m in range(1, n_tp))


def plan_stages(plan):
    depth = []
    for entry in plan:
        depth.append(0 if entry[3] is None else depth[entry[3]] + 1)
    return [[i for i, d in enumerate(depth) if d == k] for k in range(3)]


class Gather:
    def __init__(self, name, plan, buf, send, recv, tp):
        self.name = name
        self.plan, self.buf, self.send, self.recv, self.tp = plan, buf, send, recv, tp
        self.stages = plan_stages(plan)
        self.waited = set()
        self.sent = []

    def part(self, block, half):
        if half is None:
            return self.buf.at[block]
        width = self.buf.shape[-1] // 2
        return self.buf.at[block, :, pl.ds(half * width, width)]

    def copy(self, i):
        target, block, half, _ = self.plan[i]
        return pltpu.make_async_remote_copy(
            src_ref=self.part(block, half),
            dst_ref=self.part(block ^ target, half),
            send_sem=self.send.at[i],
            recv_sem=self.recv.at[i],
            device_id={"tp": self.tp ^ target},
            device_id_type=MESH,
        )

    def wait_entry(self, i):
        if i not in self.waited:
            self.waited.add(i)
            with jax.named_scope(f"w{self.name}_{i}"):
                self.copy(i).wait_recv()

    def stage(self, k):
        for i in self.stages[k]:
            if self.plan[i][3] is not None:
                self.wait_entry(self.plan[i][3])
            copy = self.copy(i)
            copy.start()
            self.sent.append(copy)

    def ready(self, block):
        for i, entry in enumerate(self.plan):
            if entry[1] ^ entry[0] == block:
                self.wait_entry(i)

    def order(self):
        blocks = [0]
        for entry in self.plan:
            if entry[0] ^ entry[1] not in blocks:
                blocks.append(entry[0] ^ entry[1])
        return blocks

    def drain(self):
        for copy in self.sent:
            copy.wait_send()


def iota(shape, axis):
    return lax.broadcasted_iota(jnp.int32, shape, axis)


def exact_dot(a, b):
    return jnp.dot(a, b, precision=lax.Precision.HIGHEST, preferred_element_type=F32)


def norm_turn(source, gain, cosine, sine):
    width = source.shape[1]
    rows = source.astype(F32)
    i0, i1 = iota((width, width), 0), iota((width, width), 1)
    same_head = jnp.where(i0 // HEAD == i1 // HEAD, 1.0 / HEAD, 0.0).astype(F32)
    mean = exact_dot(rows * rows, same_head)
    rows = rows * lax.rsqrt(mean + EPS) * gain
    partner = jnp.where(i1 % 2 == 0, i1 + 1, i1 - 1)
    sign = jnp.where(i1 % 2 == 0, -1.0, 1.0)
    swap = jnp.where(i0 == partner, sign, 0.0).astype(F32)
    return rows * cosine + exact_dot(rows, swap) * sine


def tables(cos_ref, sin_ref, offset):
    length, width = cos_ref.shape
    half_width = HEAD // 2
    inverse = THETA ** (-np.arange(0, half_width, 2, dtype=np.float32) / half_width)
    pair = iota((1, width), 1) % HEAD // 2
    row_inv = jnp.zeros((1, width), F32)
    for m, value in enumerate(inverse.astype(np.float32)):
        row_inv = jnp.where(pair % len(inverse) == m, float(value), row_inv)
    position = offset + iota((length, width), 0)
    grid = jnp.where(
        iota((length, width), 1) % HEAD < half_width, position // GRID_W, position % GRID_W
    ).astype(F32)
    angle = grid * row_inv
    cos_ref[...] = jnp.cos(angle)
    sin_ref[...] = jnp.sin(angle)


def kernel(
    n_ep, n_tp, cap, plan,
    q_ref, k_ref, v_ref, qg_ref, kg_ref, mg_ref, wo_hbm, x_ref, xg_ref,
    idst_ref, rwt_ref, wg_hbm, wu_hbm, wd_hbm,
    att_ref, mix_ref,
    cos_ref, sin_ref, xo, xb, hb, mb, kb, vb, qb, ob, rb, wgu, wd, wo,
    w_sem, v_sem,
    xz_send, xz_recv, kz_send, kz_recv, vz_send, vz_recv, rz_send, rz_recv,
    xt_send, xt_recv, ht_send, ht_recv, mt_send, mt_recv,
):
    ep, tp = lax.axis_index("ep"), lax.axis_index("tp")
    groups = xb.shape[0]
    per = n_ep // groups
    length = x_ref.shape[0]
    ffw = hb.shape[-1]

    barrier = pltpu.get_barrier_semaphore()
    for d in range(1, n_ep):
        pl.semaphore_signal(barrier, inc=1, device_id={"ep": ep ^ d}, device_id_type=MESH)
    for m in range(1, n_tp):
        pl.semaphore_signal(barrier, inc=1, device_id={"tp": tp ^ m}, device_id_type=MESH)

    lanes = (n_ep + 15) // 16 * 16
    hit_t = [(idst_ref[k : k + 1, :] == iota((lanes, length), 0)) for k in range(2)]
    both_t = sum(jnp.where(h, 1.0, 0.0) for h in hit_t).astype(BF16)
    i0, i1 = iota((length, length), 0), iota((length, length), 1)
    before_t = jnp.where(i0 < i1, 1.0, 0.0).astype(BF16)
    count_t = jnp.dot(both_t, before_t, preferred_element_type=F32)
    slot_t = [
        jnp.sum(jnp.where(hit_t[k], count_t, 0.0), axis=0, keepdims=True).astype(jnp.int32)
        + idst_ref[k : k + 1, :] * cap
        for k in range(2)
    ]

    def picked_rows(d):
        index = (ep ^ d) * cap + iota((cap, length), 0)
        choose = jnp.where((slot_t[0] == index) | (slot_t[1] == index), 1.0, 0.0).astype(BF16)
        return jnp.dot(choose, x_ref[...], preferred_element_type=F32).astype(BF16)

    sends = []

    def ep_copy(source, target, d, send, recv):
        return pltpu.make_async_remote_copy(
            src_ref=source, dst_ref=target, send_sem=send.at[d], recv_sem=recv.at[d],
            device_id={"ep": ep ^ d}, device_id_type=MESH,
        )

    def x_copy(d):
        return ep_copy(
            xo.at[d], xb.at[d // per, 0, pl.ds((d % per) * cap, cap)], d, xz_send, xz_recv
        )

    xt = [Gather(f"x{c}", plan, xb.at[c], xt_send.at[c], xt_recv.at[c], tp) for c in range(groups)]
    ht = [Gather(f"h{c}", plan, hb.at[c], ht_send.at[c], ht_recv.at[c], tp) for c in range(groups)]
    mt = Gather("m", plan, mb, mt_send, mt_recv, tp)

    xb[0, 0, pl.ds(0, cap), :] = picked_rows(0)
    pl.semaphore_wait(barrier, n_ep + n_tp - 2)
    if per == 1:
        xt[0].stage(0)

    def send_rows(c):
        for d in range(c * per, (c + 1) * per):
            if d:
                copy = x_copy(d)
                copy.start()
                sends.append(copy)

    for d in range(1, n_ep):
        xo[d] = picked_rows(d)
        if d == max(per - 1, 1):
            for c in range(0 if per > 1 else 1, 1 if per > 1 else 2):
                send_rows(c)

    def x_first(c):
        for d in range(c * per, (c + 1) * per):
            if d:
                x_copy(d).wait_recv()
        xt[c].stage(0)

    local = []
    for m in range(n_tp):
        p = tp ^ m
        pieces = (
            (wg_hbm.at[p], wgu.at[m, :, pl.ds(0, ffw)]),
            (wu_hbm.at[p], wgu.at[m, :, pl.ds(ffw, ffw)]),
            (wd_hbm.at[p], wd.at[m]),
            (wo_hbm.at[p], wo.at[m]),
        )
        for k, (source, target) in enumerate(pieces):
            copy = pltpu.make_async_copy(source, target, w_sem.at[k, m])
            copy.start()
            local.append(((k, m), copy))
    local = dict(local)
    own_v = pltpu.make_async_copy(v_ref, vb.at[0], v_sem.at[0])
    own_v.start()

    if per > 1:
        x_first(0)

    tables(cos_ref, sin_ref, ep * length)
    kb[0] = norm_turn(
        k_ref[...],
        jnp.concatenate([kg_ref[...]] * (k_ref.shape[1] // HEAD), axis=1),
        cos_ref[:, : k_ref.shape[1]],
        sin_ref[:, : k_ref.shape[1]],
    ).astype(BF16)
    own_v.wait()

    def send_keys():
        for d in range(1, n_ep):
            for source, target, send, recv in (
                (kb.at[0], kb.at[d], kz_send, kz_recv),
                (vb.at[0], vb.at[d], vz_send, vz_recv),
            ):
                copy = ep_copy(source, target, d, send, recv)
                copy.start()
                sends.append(copy)

    def turn_queries():
        qw = cos_ref.shape[1]
        gain = jnp.concatenate([qg_ref[...]] * (qw // HEAD), axis=1)
        for i in range(q_ref.shape[1] // qw):
            part = pl.ds(i * qw, qw)
            turned = norm_turn(q_ref[:, part], gain, cos_ref[...], sin_ref[...])
            qb[:, part] = (turned.astype(BF16).astype(F32) * (1.0 / math.sqrt(HEAD))).astype(BF16)

    fetched = set()

    def weights(k, m):
        if (k, m) not in fetched:
            fetched.add((k, m))
            local[k, m].wait()

    def hidden(c):
        rows = xb.shape[2]
        total = jnp.zeros((rows, 2 * ffw), F32)
        squares = jnp.zeros((rows, 1), F32)
        for m in xt[c].order():
            xt[c].ready(m)
            weights(0, m)
            weights(1, m)
            block = xb[c, m].astype(F32)
            squares += jnp.sum(block * block, axis=1, keepdims=True)
            scaled = (block * xg_ref[tp ^ m]).astype(BF16)
            total += jnp.dot(scaled, wgu[m], preferred_element_type=F32)
        stat = lax.rsqrt(squares / xg_ref.shape[0] / xg_ref.shape[2] + EPS)
        gate = total[:, :ffw] * stat
        up = total[:, ffw:] * stat
        hb[c, 0] = (gate / (1.0 + jnp.exp(-gate)) * up).astype(BF16)

    def r_copy(d):
        return ep_copy(
            ob.at[d // per, pl.ds((d % per) * cap, cap)], rb.at[d], d, rz_send, rz_recv
        )

    def down(c):
        total = jnp.zeros((ob.shape[1], ob.shape[2]), F32)
        for m in ht[c].order():
            ht[c].ready(m)
            weights(2, m)
            total += jnp.dot(hb[c, m], wd[m], preferred_element_type=F32)
        ob[c] = total.astype(BF16)
        for d in range(c * per, (c + 1) * per):
            if d:
                copy = r_copy(d)
                copy.start()
                sends.append(copy)

    def keys_ready():
        for d in range(1, n_ep):
            ep_copy(kb.at[0], kb.at[d], d, kz_send, kz_recv).wait_recv()
            ep_copy(vb.at[0], vb.at[d], d, vz_send, vz_recv).wait_recv()

    def attention(part):
        keys = n_ep * length
        block = length // 2
        rows = pl.ds(part * block, block)
        outs = []
        for h in range(q_ref.shape[1] // HEAD):
            g = h * KV_HEADS // Q_HEADS
            lane = pl.ds(g * HEAD, HEAD)
            query = qb[rows, pl.ds(h * HEAD, HEAD)]
            key = kb[:, :, lane].reshape(keys, HEAD)
            value = vb[:, :, lane].reshape(keys, HEAD)
            scores = lax.dot_general(
                query, key, (((1,), (1,)), ((), ())), preferred_element_type=F32
            )
            raw = jnp.exp(scores - jnp.max(scores, axis=1, keepdims=True))
            total = jnp.sum(raw, axis=1, keepdims=True)
            out = jnp.dot(raw.astype(BF16), value, preferred_element_type=F32)
            outs.append(out / total)
        mb[0, rows, :] = jnp.concatenate(outs, axis=1).astype(BF16)

    def project():
        total = jnp.zeros(att_ref.shape, F32)
        squares = jnp.zeros((length, 1), F32)
        for m in mt.order():
            mt.ready(m)
            weights(3, m)
            block = mb[m].astype(F32)
            squares += jnp.sum(block * block, axis=1, keepdims=True)
            scaled = (block * mg_ref[tp ^ m]).astype(BF16)
            total += jnp.dot(scaled, wo[m], preferred_element_type=F32)
        scale = lax.rsqrt(squares / mg_ref.shape[0] / mg_ref.shape[2] + EPS)
        att_ref[...] = (total * scale).astype(BF16)

    def combine():
        stack = jnp.concatenate(
            [slot_t[0].astype(F32), slot_t[1].astype(F32), rwt_ref[...]] * 2, axis=0
        )
        columns = lax.dot_general(
            jnp.where(i0 == i1, 1.0, 0.0).astype(F32), stack, (((1,), (1,)), ((), ())),
            precision=lax.Precision.HIGHEST, preferred_element_type=F32,
        )
        slot = [(columns[:, k : k + 1] + 0.5).astype(jnp.int32) for k in range(2)]
        total = [jnp.zeros(mix_ref.shape, F32) for k in range(2)]
        for d in range(n_ep):
            if d:
                r_copy(d).wait_recv()
                back = rb[d]
            else:
                back = ob[0, pl.ds(0, cap), :]
            index = (ep ^ d) * cap + iota((length, cap), 1)
            for k in range(2):
                choose = jnp.where(slot[k] == index, 1.0, 0.0).astype(BF16)
                total[k] += jnp.dot(choose, back, preferred_element_type=F32)
        mix_ref[...] = (total[0] * columns[:, 2:3] + total[1] * columns[:, 3:4]).astype(BF16)


    if per > 1:
        send_rows(1)
    send_rows(2)
    xt[0].stage(1)
    x_first(1)
    send_rows(3)
    xt[0].stage(2)
    turn_queries()
    hidden(0)
    ht[0].stage(0)
    xt[1].stage(1)
    ht[0].stage(1)
    xt[1].stage(2)
    x_first(2)
    send_keys()
    hidden(1)
    ht[1].stage(0)
    ht[0].stage(2)
    xt[2].stage(1)
    x_first(3)
    down(0)
    ht[1].stage(1)
    xt[2].stage(2)
    hidden(2)
    ht[2].stage(0)
    xt[3].stage(1)
    ht[1].stage(2)
    down(1)
    ht[2].stage(1)
    keys_ready()
    attention(0)
    xt[3].stage(2)
    ht[2].stage(2)
    hidden(3)
    ht[3].stage(0)
    down(2)
    attention(1)
    ht[3].stage(1)
    mt.stage(0)
    ht[3].stage(2)
    down(3)
    mt.stage(1)
    mt.stage(2)
    project()
    combine()

    for copy in sends:
        copy.wait_send()
    for gather in xt + ht + [mt]:
        gather.drain()


RELAY_PLAN = (
    (2, 0, 0),
    (4, 0, 1),
    (2, 0, 1),
    (4, 0, 0),
    (4, 2, 0),
    (2, 4, 1),
    (1, 0, None),
    (1, 2, None),
    (1, 4, None),
    (1, 6, None),
)
RELAY_WAIT = (0, 0, 1, 1, 2, 2, 3, 3, 3, 3)
OWN = (0, 1, 2, 3, 6)
FORWARD = (4, 5)
SIDE = (7, 8)
CORNER = (9,)
NEEDS = {FORWARD: 0, SIDE: 1, CORNER: 2}
NEAR = (0, 2, 4, 6)
FAR = (1, 3, 5, 7)


class Relay:
    def __init__(self, name, buf, send, recv, tp):
        self.name = name
        self.buf, self.send, self.recv, self.tp = buf, send, recv, tp
        self.waited = set()

    def part(self, block, half):
        if half is None:
            return self.buf.at[block]
        width = self.buf.shape[-1] // 2
        return self.buf.at[block, :, pl.ds(half * width, width)]

    def copy(self, i):
        target, block, half = RELAY_PLAN[i]
        return pltpu.make_async_remote_copy(
            src_ref=self.part(block, half),
            dst_ref=self.part(block ^ target, half),
            send_sem=self.send,
            recv_sem=self.recv.at[RELAY_WAIT[i]],
            device_id={"tp": self.tp ^ target},
            device_id_type=MESH,
        )

    def whole(self, blocks, i):
        part = self.buf.at[pl.ds(0, blocks)]
        return pltpu.make_async_remote_copy(
            src_ref=part, dst_ref=part, send_sem=self.send, recv_sem=self.recv.at[i],
            device_id={"tp": self.tp ^ 1}, device_id_type=MESH,
        )

    def wait(self, i):
        if i not in self.waited:
            self.waited.add(i)
            with jax.named_scope(f"w{self.name}_{i}"):
                self.whole(len(FAR) if i == 3 else 1, i).wait_recv()

    def issue(self, entries):
        if entries in NEEDS:
            self.wait(NEEDS[entries])
        for i in entries:
            self.copy(i).start()

    def ready(self, block):
        if block in FAR:
            self.wait(3)
        elif block:
            for i in (0, 1, 2):
                self.wait(i)

    def drain(self):
        self.whole(len(FAR) + 3, 0).wait_send()


def line_kernel(
    n_ep, n_tp, cap,
    q_ref, k_ref, v_ref, qg_ref, kg_ref, mg_ref, wo_hbm, x_ref, xg_ref,
    idst_ref, rwt_ref, wg_hbm, wu_hbm, wd_hbm,
    att_ref, mix_ref,
    cos_ref, sin_ref, xo, xb, hb, mb, kv, qb, ob, rb, ct, wgu, wd, wo,
    w_sem, z_send, z_recv, t_send, t_recv,
):
    ep, tp = lax.axis_index("ep"), lax.axis_index("tp")
    length = x_ref.shape[0]
    ffw = hb.shape[-1]
    kw = k_ref.shape[1]
    inner = (ep + 1) // 2 % 2
    order = (0, 1 + inner, 2 - inner, 3)

    barrier = pltpu.get_barrier_semaphore()
    for d in range(1, n_ep):
        pl.semaphore_signal(barrier, inc=1, device_id={"ep": ep ^ d}, device_id_type=MESH)
    for m in range(1, n_tp):
        pl.semaphore_signal(barrier, inc=1, device_id={"tp": tp ^ m}, device_id_type=MESH)

    lanes = (n_ep + 15) // 16 * 16
    hit_t = [(idst_ref[k : k + 1, :] == iota((lanes, length), 0)) for k in range(2)]
    both_t = sum(jnp.where(h, 1.0, 0.0) for h in hit_t).astype(BF16)
    i0, i1 = iota((length, length), 0), iota((length, length), 1)
    before_t = jnp.where(i0 < i1, 1.0, 0.0).astype(BF16)
    count_t = jnp.dot(both_t, before_t, preferred_element_type=F32)
    slot_t = [
        jnp.sum(jnp.where(hit_t[k], count_t, 0.0), axis=0, keepdims=True).astype(jnp.int32)
        + idst_ref[k : k + 1, :] * cap
        for k in range(2)
    ]

    def picked_rows(d):
        index = (ep ^ d) * cap + iota((cap, length), 0)
        choose = jnp.where((slot_t[0] == index) | (slot_t[1] == index), 1.0, 0.0).astype(BF16)
        return jnp.dot(choose, x_ref[...], preferred_element_type=F32).astype(BF16)

    def ep_copy(source, target, d, send, recv):
        return pltpu.make_async_remote_copy(
            src_ref=source, dst_ref=target, send_sem=send, recv_sem=recv,
            device_id={"ep": ep ^ d}, device_id_type=MESH,
        )

    def x_copy(d):
        return ep_copy(xo.at[d], xb.at[d, 0], d, z_send.at[0], z_recv.at[0, d])

    def r_copy(d):
        return ep_copy(ob.at[d], rb.at[d], d, z_send.at[1], z_recv.at[1, d])

    def kv_copy(i):
        d, block = ((1, 0), (2, 0), (1, 2))[i]
        return ep_copy(kv.at[block], kv.at[block ^ d], d, z_send.at[2], z_recv.at[2, i])

    xt = [
        Relay(f"x{j}", xb.at[order[j]], t_send.at[0, order[j]], t_recv.at[0, order[j]], tp)
        for j in range(n_ep)
    ]
    ht = [
        Relay(f"h{d}", hb.at[d], t_send.at[1, d], t_recv.at[1, d], tp)
        for d in range(n_ep)
    ]
    mt = Relay("m", mb, t_send.at[2, 0], t_recv.at[2, 0], tp)

    pieces = (
        (wg_hbm, wgu.at[:, :, pl.ds(0, ffw)]),
        (wu_hbm, wgu.at[:, :, pl.ds(ffw, ffw)]),
        (wd_hbm, wd),
        (wo_hbm, wo),
    )
    local = [
        pltpu.make_async_copy(source, target, w_sem.at[k])
        for k, (source, target) in enumerate(pieces)
    ]
    fetched = set()

    def weights(k):
        if k not in fetched:
            fetched.add(k)
            with jax.named_scope(f"ww_{k}"):
                local[k].wait()

    def own_keys():
        tables(cos_ref, sin_ref, ep * length)
        kv[0, :, pl.ds(kw, kw)] = v_ref[...]
        kv[0, :, pl.ds(0, kw)] = norm_turn(
            k_ref[...],
            jnp.concatenate([kg_ref[...]] * (kw // HEAD), axis=1),
            cos_ref[:, :kw],
            sin_ref[:, :kw],
        ).astype(BF16)

    def send_keys():
        kv_copy(0).start()
        kv_copy(1).start()

    def keys_on():
        with jax.named_scope("wkv_1"):
            kv_copy(1).wait_recv()
        kv_copy(2).start()

    def keys_ready():
        with jax.named_scope("wkv_0"):
            kv_copy(0).wait_recv()
        with jax.named_scope("wkv_2"):
            kv_copy(2).wait_recv()

    def turn_queries():
        qw = cos_ref.shape[1]
        gain = jnp.concatenate([qg_ref[...]] * (qw // HEAD), axis=1)
        for i in range(q_ref.shape[1] // qw):
            part = pl.ds(i * qw, qw)
            turned = norm_turn(q_ref[:, part], gain, cos_ref[...], sin_ref[...])
            qb[:, part] = (turned.astype(BF16).astype(F32) * (1.0 / math.sqrt(HEAD))).astype(BF16)

    def x_arrived(j):
        with jax.named_scope(f"wxz_{j}"):
            x_copy(order[j]).wait_recv()

    def hidden(j):
        d = order[j]
        total = jnp.zeros((cap, 2 * ffw), F32)
        squares = jnp.zeros((cap, 1), F32)
        for m in NEAR + FAR:
            xt[j].ready(m)
            weights(0)
            weights(1)
            block = xb[d, m].astype(F32)
            squares += jnp.sum(block * block, axis=1, keepdims=True)
            scaled = (block * xg_ref[tp ^ m]).astype(BF16)
            total += jnp.dot(scaled, wgu[tp ^ m], preferred_element_type=F32)
        stat = lax.rsqrt(squares / xg_ref.shape[0] / xg_ref.shape[2] + EPS)
        gate = total[:, :ffw] * stat
        up = total[:, ffw:] * stat
        hb[d, 0] = (gate / (1.0 + jnp.exp(-gate)) * up).astype(BF16)

    def down(d):
        total = jnp.zeros((ob.shape[1], ob.shape[2]), F32)
        for m in NEAR + FAR:
            ht[d].ready(m)
            weights(2)
            total += jnp.dot(hb[d, m], wd[tp ^ m], preferred_element_type=F32)
        ob[d] = total.astype(BF16)
        if d:
            r_copy(d).start()

    def attention(part, pair):
        keys = n_ep * length
        block = length // 2
        rows = pl.ds(part * block, block)
        outs = []
        for h in range(2 * pair, 2 * pair + 2):
            g = h * KV_HEADS // Q_HEADS
            query = qb[rows, pl.ds(h * HEAD, HEAD)]
            key = kv[:, :, pl.ds(g * HEAD, HEAD)].reshape(keys, HEAD)
            value = kv[:, :, pl.ds(kw + g * HEAD, HEAD)].reshape(keys, HEAD)
            scores = lax.dot_general(
                query, key, (((1,), (1,)), ((), ())), preferred_element_type=F32
            )
            raw = jnp.exp(scores - jnp.max(scores, axis=1, keepdims=True))
            total = jnp.sum(raw, axis=1, keepdims=True)
            out = jnp.dot(raw.astype(BF16), value, preferred_element_type=F32)
            outs.append(out / total)
        lane = pl.ds(2 * pair * HEAD, 2 * HEAD)
        mb[0, rows, lane] = jnp.concatenate(outs, axis=1).astype(BF16)

    def project():
        total = jnp.zeros(att_ref.shape, F32)
        squares = jnp.zeros((length, 1), F32)
        for m in NEAR + FAR:
            mt.ready(m)
            weights(3)
            block = mb[m].astype(F32)
            squares += jnp.sum(block * block, axis=1, keepdims=True)
            scaled = (block * mg_ref[tp ^ m]).astype(BF16)
            total += jnp.dot(scaled, wo[tp ^ m], preferred_element_type=F32)
        scale = lax.rsqrt(squares / mg_ref.shape[0] / mg_ref.shape[2] + EPS)
        att_ref[...] = (total * scale).astype(BF16)

    places = {}

    def columns():
        stack = jnp.concatenate(
            [slot_t[0].astype(F32), slot_t[1].astype(F32), rwt_ref[...]] * 2, axis=0
        )
        column = lax.dot_general(
            jnp.where(i0 == i1, 1.0, 0.0).astype(F32), stack, (((1,), (1,)), ((), ())),
            precision=lax.Precision.HIGHEST, preferred_element_type=F32,
        )
        places["slot"] = [(column[:, k : k + 1] + 0.5).astype(jnp.int32) for k in range(2)]
        places["weight"] = [column[:, 2 + k : 3 + k] for k in range(2)]

    def combine(d, first=False, last=False):
        if d:
            with jax.named_scope(f"wr_{d}"):
                r_copy(d).wait_recv()
        back = rb[d] if d else ob[0]
        index = (ep ^ d) * cap + iota((length, cap), 1)
        total = []
        for k in range(2):
            choose = jnp.where(places["slot"][k] == index, 1.0, 0.0).astype(BF16)
            found = jnp.dot(choose, back, preferred_element_type=F32)
            total.append(found if first else ct[k] + found)
        if last:
            weight = places["weight"]
            mix_ref[...] = (total[0] * weight[0] + total[1] * weight[1]).astype(BF16)
        else:
            for k in range(2):
                ct[k] = total[k]

    def step(name, f, *args, **kwargs):
        with jax.named_scope("S_" + name):
            f(*args, **kwargs)

    def send_x(d):
        xo[d] = picked_rows(d)
        x_copy(d).start()

    for copy in local:
        copy.start()
    xb[0, 0] = picked_rows(0)
    with jax.named_scope("S_barrier"):
        pl.semaphore_wait(barrier, n_ep + n_tp - 2)
    step("X0own", xt[0].issue, OWN)
    step("sx2", send_x, 2)
    step("sx1", send_x, 1)
    step("keys", own_keys)
    step("X0fwd", xt[0].issue, FORWARD)
    step("X0side", xt[0].issue, SIDE)
    step("columns", columns)
    step("ax1", x_arrived, 1)
    step("X1own", xt[1].issue, OWN)
    step("sx3", send_x, 3)
    step("X0cor", xt[0].issue, CORNER)
    step("hid0", hidden, 0)
    step("X1fwd", xt[1].issue, FORWARD)
    step("ax2", x_arrived, 2)
    step("X2own", xt[2].issue, OWN)
    step("X1side", xt[1].issue, SIDE)
    step("X1cor", xt[1].issue, CORNER)
    step("X2fwd", xt[2].issue, FORWARD)
    step("ax3", x_arrived, 3)
    step("X3own", xt[3].issue, OWN)
    step("hid1", hidden, 1)
    step("sendkv", send_keys)
    step("X2side", xt[2].issue, SIDE)
    step("queries", turn_queries)
    step("X2cor", xt[2].issue, CORNER)
    step("X3fwd", xt[3].issue, FORWARD)
    step("hid2", hidden, 2)
    step("H2own", ht[2].issue, OWN)
    step("H1own", ht[1].issue, OWN)
    step("X3side", xt[3].issue, SIDE)
    step("X3cor", xt[3].issue, CORNER)
    step("keyson", keys_on)
    step("H2fwd", ht[2].issue, FORWARD)
    step("hid3", hidden, 3)
    step("H3own", ht[3].issue, OWN)
    step("H1fwd", ht[1].issue, FORWARD)
    step("H2side", ht[2].issue, SIDE)
    step("H2cor", ht[2].issue, CORNER)
    step("wkv", keys_ready)
    step("att00", attention, 0, 0)
    step("att01", attention, 0, 1)
    step("H3fwd", ht[3].issue, FORWARD)
    step("down2", down, 2)
    step("att10", attention, 1, 0)
    step("H1side", ht[1].issue, SIDE)
    step("H1cor", ht[1].issue, CORNER)
    step("att11", attention, 1, 1)
    step("Mown", mt.issue, OWN)
    step("H3side", ht[3].issue, SIDE)
    step("down1", down, 1)
    step("H3cor", ht[3].issue, CORNER)
    step("H0own", ht[0].issue, OWN)
    step("down3", down, 3)
    step("Mfwd", mt.issue, FORWARD)
    step("Mside", mt.issue, SIDE)
    step("H0fwd", ht[0].issue, FORWARD)
    step("Mcor", mt.issue, CORNER)
    step("H0side", ht[0].issue, SIDE)
    step("H0cor", ht[0].issue, CORNER)
    step("project", project)
    step("down0", down, 0)
    step("comb0F", combine, 0, first=True)
    step("comb1", combine, 1)
    step("comb2", combine, 2)
    step("comb3L", combine, 3, last=True)

    with jax.named_scope("S_drain"):
        for i, buf in enumerate((xo, rb, kv)):
            ep_copy(
                buf.at[pl.ds(0, n_ep - 1)], buf.at[pl.ds(0, n_ep - 1)], 1,
                z_send.at[i], z_recv.at[i, 0],
            ).wait_send()
        for gather in xt + ht + [mt]:
            gather.drain()


def hand_on(a_ref, b_ref, a_out, b_out):
    a_out[...] = a_ref[...]
    b_out[...] = b_ref[...]


def shards(
    n_ep, n_tp,
    queries, key_rows, values, query_gain, key_gain, mix_gain, out_weight, expert_input,
    expert_gain, route_ids, route_weights, expert_gate, expert_up, expert_down,
):
    length, width = expert_input.shape
    qw, kw = queries.shape[1], key_rows.shape[1]
    ffw = expert_gate.shape[2]
    out_w = out_weight.shape[1]
    copies = length * route_ids.shape[1]
    capacity = (4 * copies + 3 * n_ep - 1) // (3 * n_ep)
    cap = (capacity + 15) // 16 * 16
    groups = 4
    rows = cap * (n_ep // groups)
    plan = gather_plan(n_tp)

    table_w = min(128, qw)
    operands = (
        queries, key_rows, values,
        query_gain.reshape(1, HEAD), key_gain.reshape(1, HEAD),
        mix_gain.reshape(n_tp, 1, qw),
        out_weight.reshape(n_tp, qw, out_w),
        expert_input,
        expert_gain.reshape(n_tp, 1, width),
        route_ids.T, route_weights.T,
        expert_gate.reshape(n_tp, width, ffw),
        expert_up.reshape(n_tp, width, ffw),
        expert_down.reshape(n_tp, ffw, out_w),
    )
    vmem = pl.BlockSpec(memory_space=pltpu.VMEM)
    hbm = pl.BlockSpec(memory_space=pl.ANY)
    specs = [hbm if i in (6, 11, 12, 13) else vmem for i in range(len(operands))]
    dma = pltpu.SemaphoreType.DMA
    line = n_ep == 4 and n_tp == 8
    tables_at = [pltpu.VMEM((length, table_w), F32)] * 2
    blocks_at = [
        pltpu.VMEM((n_ep, cap, width), BF16),
        pltpu.VMEM((groups, n_tp, rows, width), BF16),
        pltpu.VMEM((groups, n_tp, rows, ffw), BF16),
        pltpu.VMEM((n_tp, length, qw), BF16),
    ]
    weights_at = [
        pltpu.VMEM((n_tp, width, 2 * ffw), BF16),
        pltpu.VMEM((n_tp, ffw, out_w), BF16),
        pltpu.VMEM((n_tp, qw, out_w), BF16),
    ]
    results_at = [
        pltpu.VMEM((length, qw), BF16),
        pltpu.VMEM((groups, rows, out_w), BF16),
        pltpu.VMEM((n_ep, cap, out_w), BF16),
    ]
    if line:
        body = functools.partial(line_kernel, n_ep, n_tp, cap)
        scratch = tables_at + blocks_at + [pltpu.VMEM((n_ep, length, 2 * kw), BF16)]
        scratch += results_at + [pltpu.VMEM((2, length, out_w), F32)] + weights_at
        scratch += [dma((4,)), dma((3,)), dma((3, n_ep)), dma((3, n_ep)), dma((3, n_ep, 4))]
    else:
        body = functools.partial(kernel, n_ep, n_tp, cap, plan)
        scratch = tables_at + blocks_at + [pltpu.VMEM((n_ep, length, kw), BF16)] * 2
        scratch += results_at + weights_at
        scratch += [dma((4, n_tp)), dma((1,))] + [dma((n_ep,))] * 8
        scratch += [dma((groups, len(plan)))] * 4 + [dma((len(plan),))] * 2
    outs = pl.pallas_call(
        body,
        out_shape=(
            jax.ShapeDtypeStruct((length, out_w), BF16),
            jax.ShapeDtypeStruct((length, out_w), BF16),
        ),
        in_specs=specs,
        out_specs=(vmem, vmem),
        scratch_shapes=scratch,
        compiler_params=pltpu.CompilerParams(
            collective_id=0, has_side_effects=True, vmem_limit_bytes=60 * 1024 * 1024
        ),
    )(*operands)
    return pl.pallas_call(
        hand_on,
        out_shape=tuple(jax.ShapeDtypeStruct(o.shape, o.dtype) for o in outs),
        in_specs=(vmem, vmem),
        out_specs=(vmem, vmem),
    )(*outs)


def solution(mesh):
    placed = (
        P("ep", "tp"), P("ep", "tp"), P("ep", "tp"), P(), P(), P(), P(None, "tp"),
        P("ep", "tp"), P(), P("ep", None), P("ep", None),
        P("ep", None, "tp"), P("ep", None, "tp"), P("ep", None, "tp"),
    )
    return jax.shard_map(
        functools.partial(shards, mesh.shape["ep"], mesh.shape["tp"]),
        mesh=mesh,
        in_specs=placed,
        out_specs=(P("ep", "tp"), P("ep", "tp")),
        check_vma=False,
    )
```

```python
import functools
import math
import types

import jax
import jax.numpy as jnp
import numpy as np
from jax import lax
from jax.experimental import pallas as pl
from jax.experimental.pallas import tpu as pltpu
from jax.sharding import PartitionSpec as P

Q_HEADS = 32
KV_HEADS = 16
HEAD = 64
GRID_W = 64
EPS = 1e-06
THETA = 10000.0
MESH = pl.DeviceIdType.MESH
F32 = jnp.float32
BF16 = jnp.bfloat16


def gather_plan(n_tp):
    if n_tp == 8:
        return (
            (2, 0, None, None),
            (4, 0, None, None),
            (1, 0, None, None),
            (4, 2, 0, 0),
            (2, 4, 1, 1),
            (1, 2, None, 0),
            (1, 4, None, 1),
            (1, 6, 0, 3),
            (1, 6, 1, 4),
        )
    return tuple((m, 0, None, None) for m in range(1, n_tp))


def plan_stages(plan):
    depth = []
    for entry in plan:
        depth.append(0 if entry[3] is None else depth[entry[3]] + 1)
    return [[i for i, d in enumerate(depth) if d == k] for k in range(3)]


class Gather:
    def __init__(self, name, plan, buf, send, recv, tp):
        self.name = name
        self.plan, self.buf, self.send, self.recv, self.tp = plan, buf, send, recv, tp
        self.stages = plan_stages(plan)
        self.waited = set()
        self.sent = []

    def part(self, block, half):
        if half is None:
            return self.buf.at[block]
        width = self.buf.shape[-1] // 2
        return self.buf.at[block, :, pl.ds(half * width, width)]

    def copy(self, i):
        target, block, half, _ = self.plan[i]
        return pltpu.make_async_remote_copy(
            src_ref=self.part(block, half),
            dst_ref=self.part(block ^ target, half),
            send_sem=self.send.at[i],
            recv_sem=self.recv.at[i],
            device_id={"tp": self.tp ^ target},
            device_id_type=MESH,
        )

    def wait_entry(self, i):
        if i not in self.waited:
            self.waited.add(i)
            with jax.named_scope(f"w{self.name}_{i}"):
                self.copy(i).wait_recv()

    def stage(self, k):
        for i in self.stages[k]:
            if self.plan[i][3] is not None:
                self.wait_entry(self.plan[i][3])
            copy = self.copy(i)
            copy.start()
            self.sent.append(copy)

    def ready(self, block):
        for i, entry in enumerate(self.plan):
            if entry[1] ^ entry[0] == block:
                self.wait_entry(i)

    def order(self):
        blocks = [0]
        for entry in self.plan:
            if entry[0] ^ entry[1] not in blocks:
                blocks.append(entry[0] ^ entry[1])
        return blocks

    def drain(self):
        for copy in self.sent:
            copy.wait_send()


def iota(shape, axis):
    return lax.broadcasted_iota(jnp.int32, shape, axis)


def exact_dot(a, b):
    return jnp.dot(a, b, precision=lax.Precision.HIGHEST, preferred_element_type=F32)


def norm_turn(source, gain, cosine, sine):
    width = source.shape[1]
    rows = source.astype(F32)
    i0, i1 = iota((width, width), 0), iota((width, width), 1)
    same_head = jnp.where(i0 // HEAD == i1 // HEAD, 1.0 / HEAD, 0.0).astype(F32)
    mean = exact_dot(rows * rows, same_head)
    rows = rows * lax.rsqrt(mean + EPS) * gain
    partner = jnp.where(i1 % 2 == 0, i1 + 1, i1 - 1)
    sign = jnp.where(i1 % 2 == 0, -1.0, 1.0)
    swap = jnp.where(i0 == partner, sign, 0.0).astype(F32)
    return rows * cosine + exact_dot(rows, swap) * sine


def tables(cos_ref, sin_ref, offset):
    length, width = cos_ref.shape
    half_width = HEAD // 2
    inverse = THETA ** (-np.arange(0, half_width, 2, dtype=np.float32) / half_width)
    pair = iota((1, width), 1) % HEAD // 2
    row_inv = jnp.zeros((1, width), F32)
    for m, value in enumerate(inverse.astype(np.float32)):
        row_inv = jnp.where(pair % len(inverse) == m, float(value), row_inv)
    position = offset + iota((length, width), 0)
    grid = jnp.where(
        iota((length, width), 1) % HEAD < half_width, position // GRID_W, position % GRID_W
    ).astype(F32)
    angle = grid * row_inv
    cos_ref[...] = jnp.cos(angle)
    sin_ref[...] = jnp.sin(angle)


def kernel(
    n_ep, n_tp, cap, plan,
    q_ref, k_ref, v_ref, qg_ref, kg_ref, mg_ref, wo_hbm, x_ref, xg_ref,
    idst_ref, rwt_ref, wg_hbm, wu_hbm, wd_hbm,
    att_ref, mix_ref,
    cos_ref, sin_ref, xo, xb, hb, mb, kb, vb, qb, ob, rb, wgu, wd, wo,
    w_sem, v_sem,
    xz_send, xz_recv, kz_send, kz_recv, vz_send, vz_recv, rz_send, rz_recv,
    xt_send, xt_recv, ht_send, ht_recv, mt_send, mt_recv,
):
    ep, tp = lax.axis_index("ep"), lax.axis_index("tp")
    groups = xb.shape[0]
    per = n_ep // groups
    length = x_ref.shape[0]
    ffw = hb.shape[-1]

    barrier = pltpu.get_barrier_semaphore()
    for d in range(1, n_ep):
        pl.semaphore_signal(barrier, inc=1, device_id={"ep": ep ^ d}, device_id_type=MESH)
    for m in range(1, n_tp):
        pl.semaphore_signal(barrier, inc=1, device_id={"tp": tp ^ m}, device_id_type=MESH)

    lanes = (n_ep + 15) // 16 * 16
    hit_t = [(idst_ref[k : k + 1, :] == iota((lanes, length), 0)) for k in range(2)]
    both_t = sum(jnp.where(h, 1.0, 0.0) for h in hit_t).astype(BF16)
    i0, i1 = iota((length, length), 0), iota((length, length), 1)
    before_t = jnp.where(i0 < i1, 1.0, 0.0).astype(BF16)
    count_t = jnp.dot(both_t, before_t, preferred_element_type=F32)
    slot_t = [
        jnp.sum(jnp.where(hit_t[k], count_t, 0.0), axis=0, keepdims=True).astype(jnp.int32)
        + idst_ref[k : k + 1, :] * cap
        for k in range(2)
    ]

    def picked_rows(d):
        index = (ep ^ d) * cap + iota((cap, length), 0)
        choose = jnp.where((slot_t[0] == index) | (slot_t[1] == index), 1.0, 0.0).astype(BF16)
        return jnp.dot(choose, x_ref[...], preferred_element_type=F32).astype(BF16)

    sends = []

    def ep_copy(source, target, d, send, recv):
        return pltpu.make_async_remote_copy(
            src_ref=source, dst_ref=target, send_sem=send.at[d], recv_sem=recv.at[d],
            device_id={"ep": ep ^ d}, device_id_type=MESH,
        )

    def x_copy(d):
        return ep_copy(
            xo.at[d], xb.at[d // per, 0, pl.ds((d % per) * cap, cap)], d, xz_send, xz_recv
        )

    xt = [Gather(f"x{c}", plan, xb.at[c], xt_send.at[c], xt_recv.at[c], tp) for c in range(groups)]
    ht = [Gather(f"h{c}", plan, hb.at[c], ht_send.at[c], ht_recv.at[c], tp) for c in range(groups)]
    mt = Gather("m", plan, mb, mt_send, mt_recv, tp)

    xb[0, 0, pl.ds(0, cap), :] = picked_rows(0)
    pl.semaphore_wait(barrier, n_ep + n_tp - 2)
    if per == 1:
        xt[0].stage(0)

    def send_rows(c):
        for d in range(c * per, (c + 1) * per):
            if d:
                copy = x_copy(d)
                copy.start()
                sends.append(copy)

    for d in range(1, n_ep):
        xo[d] = picked_rows(d)
        if d == max(per - 1, 1):
            for c in range(0 if per > 1 else 1, 1 if per > 1 else 2):
                send_rows(c)

    def x_first(c):
        for d in range(c * per, (c + 1) * per):
            if d:
                x_copy(d).wait_recv()
        xt[c].stage(0)

    local = []
    for m in range(n_tp):
        p = tp ^ m
        pieces = (
            (wg_hbm.at[p], wgu.at[m, :, pl.ds(0, ffw)]),
            (wu_hbm.at[p], wgu.at[m, :, pl.ds(ffw, ffw)]),
            (wd_hbm.at[p], wd.at[m]),
            (wo_hbm.at[p], wo.at[m]),
        )
        for k, (source, target) in enumerate(pieces):
            copy = pltpu.make_async_copy(source, target, w_sem.at[k, m])
            copy.start()
            local.append(((k, m), copy))
    local = dict(local)
    own_v = pltpu.make_async_copy(v_ref, vb.at[0], v_sem.at[0])
    own_v.start()

    if per > 1:
        x_first(0)

    tables(cos_ref, sin_ref, ep * length)
    kb[0] = norm_turn(
        k_ref[...],
        jnp.concatenate([kg_ref[...]] * (k_ref.shape[1] // HEAD), axis=1),
        cos_ref[:, : k_ref.shape[1]],
        sin_ref[:, : k_ref.shape[1]],
    ).astype(BF16)
    own_v.wait()

    def send_keys():
        for d in range(1, n_ep):
            for source, target, send, recv in (
                (kb.at[0], kb.at[d], kz_send, kz_recv),
                (vb.at[0], vb.at[d], vz_send, vz_recv),
            ):
                copy = ep_copy(source, target, d, send, recv)
                copy.start()
                sends.append(copy)

    def turn_queries():
        qw = cos_ref.shape[1]
        gain = jnp.concatenate([qg_ref[...]] * (qw // HEAD), axis=1)
        for i in range(q_ref.shape[1] // qw):
            part = pl.ds(i * qw, qw)
            turned = norm_turn(q_ref[:, part], gain, cos_ref[...], sin_ref[...])
            qb[:, part] = (turned.astype(BF16).astype(F32) * (1.0 / math.sqrt(HEAD))).astype(BF16)

    fetched = set()

    def weights(k, m):
        if (k, m) not in fetched:
            fetched.add((k, m))
            local[k, m].wait()

    def hidden(c):
        rows = xb.shape[2]
        total = jnp.zeros((rows, 2 * ffw), F32)
        squares = jnp.zeros((rows, 1), F32)
        for m in xt[c].order():
            xt[c].ready(m)
            weights(0, m)
            weights(1, m)
            block = xb[c, m].astype(F32)
            squares += jnp.sum(block * block, axis=1, keepdims=True)
            scaled = (block * xg_ref[tp ^ m]).astype(BF16)
            total += jnp.dot(scaled, wgu[m], preferred_element_type=F32)
        stat = lax.rsqrt(squares / xg_ref.shape[0] / xg_ref.shape[2] + EPS)
        gate = total[:, :ffw] * stat
        up = total[:, ffw:] * stat
        hb[c, 0] = (gate / (1.0 + jnp.exp(-gate)) * up).astype(BF16)

    def r_copy(d):
        return ep_copy(
            ob.at[d // per, pl.ds((d % per) * cap, cap)], rb.at[d], d, rz_send, rz_recv
        )

    def down(c):
        total = jnp.zeros((ob.shape[1], ob.shape[2]), F32)
        for m in ht[c].order():
            ht[c].ready(m)
            weights(2, m)
            total += jnp.dot(hb[c, m], wd[m], preferred_element_type=F32)
        ob[c] = total.astype(BF16)
        for d in range(c * per, (c + 1) * per):
            if d:
                copy = r_copy(d)
                copy.start()
                sends.append(copy)

    def keys_ready():
        for d in range(1, n_ep):
            ep_copy(kb.at[0], kb.at[d], d, kz_send, kz_recv).wait_recv()
            ep_copy(vb.at[0], vb.at[d], d, vz_send, vz_recv).wait_recv()

    def attention(part):
        keys = n_ep * length
        block = length // 2
        rows = pl.ds(part * block, block)
        outs = []
        for h in range(q_ref.shape[1] // HEAD):
            g = h * KV_HEADS // Q_HEADS
            lane = pl.ds(g * HEAD, HEAD)
            query = qb[rows, pl.ds(h * HEAD, HEAD)]
            key = kb[:, :, lane].reshape(keys, HEAD)
            value = vb[:, :, lane].reshape(keys, HEAD)
            scores = lax.dot_general(
                query, key, (((1,), (1,)), ((), ())), preferred_element_type=F32
            )
            raw = jnp.exp(scores - jnp.max(scores, axis=1, keepdims=True))
            total = jnp.sum(raw, axis=1, keepdims=True)
            out = jnp.dot(raw.astype(BF16), value, preferred_element_type=F32)
            outs.append(out / total)
        mb[0, rows, :] = jnp.concatenate(outs, axis=1).astype(BF16)

    def project():
        total = jnp.zeros(att_ref.shape, F32)
        squares = jnp.zeros((length, 1), F32)
        for m in mt.order():
            mt.ready(m)
            weights(3, m)
            block = mb[m].astype(F32)
            squares += jnp.sum(block * block, axis=1, keepdims=True)
            scaled = (block * mg_ref[tp ^ m]).astype(BF16)
            total += jnp.dot(scaled, wo[m], preferred_element_type=F32)
        scale = lax.rsqrt(squares / mg_ref.shape[0] / mg_ref.shape[2] + EPS)
        att_ref[...] = (total * scale).astype(BF16)

    def combine():
        stack = jnp.concatenate(
            [slot_t[0].astype(F32), slot_t[1].astype(F32), rwt_ref[...]] * 2, axis=0
        )
        columns = lax.dot_general(
            jnp.where(i0 == i1, 1.0, 0.0).astype(F32), stack, (((1,), (1,)), ((), ())),
            precision=lax.Precision.HIGHEST, preferred_element_type=F32,
        )
        slot = [(columns[:, k : k + 1] + 0.5).astype(jnp.int32) for k in range(2)]
        total = [jnp.zeros(mix_ref.shape, F32) for k in range(2)]
        for d in range(n_ep):
            if d:
                r_copy(d).wait_recv()
                back = rb[d]
            else:
                back = ob[0, pl.ds(0, cap), :]
            index = (ep ^ d) * cap + iota((length, cap), 1)
            for k in range(2):
                choose = jnp.where(slot[k] == index, 1.0, 0.0).astype(BF16)
                total[k] += jnp.dot(choose, back, preferred_element_type=F32)
        mix_ref[...] = (total[0] * columns[:, 2:3] + total[1] * columns[:, 3:4]).astype(BF16)


    if per > 1:
        send_rows(1)
    send_rows(2)
    xt[0].stage(1)
    x_first(1)
    send_rows(3)
    xt[0].stage(2)
    turn_queries()
    hidden(0)
    ht[0].stage(0)
    xt[1].stage(1)
    ht[0].stage(1)
    xt[1].stage(2)
    x_first(2)
    send_keys()
    hidden(1)
    ht[1].stage(0)
    ht[0].stage(2)
    xt[2].stage(1)
    x_first(3)
    down(0)
    ht[1].stage(1)
    xt[2].stage(2)
    hidden(2)
    ht[2].stage(0)
    xt[3].stage(1)
    ht[1].stage(2)
    down(1)
    ht[2].stage(1)
    keys_ready()
    attention(0)
    xt[3].stage(2)
    ht[2].stage(2)
    hidden(3)
    ht[3].stage(0)
    down(2)
    attention(1)
    ht[3].stage(1)
    mt.stage(0)
    ht[3].stage(2)
    down(3)
    mt.stage(1)
    mt.stage(2)
    project()
    combine()

    for copy in sends:
        copy.wait_send()
    for gather in xt + ht + [mt]:
        gather.drain()


RELAY_PLAN = (
    (2, 0, 0),
    (4, 0, 1),
    (2, 0, 1),
    (4, 0, 0),
    (4, 2, 0),
    (2, 4, 1),
    (1, 0, None),
    (1, 2, None),
    (1, 4, None),
    (1, 6, None),
)
RELAY_WAIT = (0, 0, 1, 1, 2, 2, 3, 3, 3, 3)
OWN = (0, 1, 2, 3, 6)
LEAD = (0, 1)
REST = (2, 3, 6)
FORWARD = (4, 5)
SIDE = (7, 8)
CORNER = (9,)
NEEDS = {FORWARD: 0, SIDE: 1, CORNER: 2}
NEAR = (0, 2, 4, 6)
FAR = (1, 3, 5, 7)


class Relay:
    def __init__(self, name, buf, send, recv, tp):
        self.name = name
        self.buf, self.send, self.recv, self.tp = buf, send, recv, tp
        self.waited = set()

    def part(self, block, half):
        if half is None:
            return self.buf.at[block]
        width = self.buf.shape[-1] // 2
        return self.buf.at[block, :, pl.ds(half * width, width)]

    def copy(self, i):
        target, block, half = RELAY_PLAN[i]
        return pltpu.make_async_remote_copy(
            src_ref=self.part(block, half),
            dst_ref=self.part(block ^ target, half),
            send_sem=self.send,
            recv_sem=self.recv.at[RELAY_WAIT[i]],
            device_id={"tp": self.tp ^ target},
            device_id_type=MESH,
        )

    def whole(self, blocks, i):
        part = self.buf.at[pl.ds(0, blocks)]
        return pltpu.make_async_remote_copy(
            src_ref=part, dst_ref=part, send_sem=self.send, recv_sem=self.recv.at[i],
            device_id={"tp": self.tp ^ 1}, device_id_type=MESH,
        )

    def wait(self, i):
        if i not in self.waited:
            self.waited.add(i)
            with jax.named_scope(f"w{self.name}_{i}"):
                self.whole(len(FAR) if i == 3 else 1, i).wait_recv()

    def issue(self, entries):
        if entries in NEEDS:
            self.wait(NEEDS[entries])
        for i in entries:
            self.copy(i).start()

    def ready(self, block):
        if block in FAR:
            self.wait(3)
        elif block:
            for i in (0, 1, 2):
                self.wait(i)

    def drain(self):
        self.whole(len(FAR) + 3, 0).wait_send()


def line_kernel(
    n_ep, n_tp, cap,
    q_ref, k_ref, v_ref, qg_ref, kg_ref, mg_ref, wo_hbm, x_ref, xg_ref,
    idst_ref, rwt_ref, wg_hbm, wu_hbm, wd_hbm,
    att_ref, mix_ref,
    cos_ref, sin_ref, xo, xb, hb, mb, kv, qb, ob, rb, ct, wgu, wd, wo,
    w_sem, z_send, z_recv, t_send, t_recv,
):
    ep, tp = lax.axis_index("ep"), lax.axis_index("tp")
    length = x_ref.shape[0]
    ffw = hb.shape[-1]
    kw = k_ref.shape[1]
    half = length // 2
    inner = (ep + 1) // 2 % 2

    barrier = pltpu.get_barrier_semaphore()
    for d in range(1, n_ep):
        pl.semaphore_signal(barrier, inc=1, device_id={"ep": ep ^ d}, device_id_type=MESH)
    for m in range(1, n_tp):
        pl.semaphore_signal(barrier, inc=1, device_id={"tp": tp ^ m}, device_id_type=MESH)

    lanes = (n_ep + 15) // 16 * 16
    hit_t = [(idst_ref[k : k + 1, :] == iota((lanes, length), 0)) for k in range(2)]
    both_t = sum(jnp.where(h, 1.0, 0.0) for h in hit_t).astype(BF16)
    i0, i1 = iota((length, length), 0), iota((length, length), 1)
    before_t = jnp.where(i0 < i1, 1.0, 0.0).astype(BF16)
    count_t = jnp.dot(both_t, before_t, preferred_element_type=F32)
    slot_t = [
        jnp.sum(jnp.where(hit_t[k], count_t, 0.0), axis=0, keepdims=True).astype(jnp.int32)
        + idst_ref[k : k + 1, :] * cap
        for k in range(2)
    ]

    def picked_rows(d):
        index = (ep ^ d) * cap + iota((cap, length), 0)
        choose = jnp.where((slot_t[0] == index) | (slot_t[1] == index), 1.0, 0.0).astype(BF16)
        return jnp.dot(choose, x_ref[...], preferred_element_type=F32).astype(BF16)

    def ep_copy(source, target, d, send, recv):
        return pltpu.make_async_remote_copy(
            src_ref=source, dst_ref=target, send_sem=send, recv_sem=recv,
            device_id={"ep": ep ^ d}, device_id_type=MESH,
        )

    def x_copy(d):
        return ep_copy(xo.at[d], xb.at[d, 0], d, z_send.at[0], z_recv.at[0, d])

    def r_copy(d):
        return ep_copy(ob.at[d], rb.at[d], d, z_send.at[1], z_recv.at[1, d])

    def kv_copy(i):
        d, block = ((1, 0), (2, 0), (1, 2))[i]
        return ep_copy(kv.at[block], kv.at[block ^ d], d, z_send.at[2], z_recv.at[2, i])

    live = types.SimpleNamespace()

    def fresh():
        live.fetched = set()
        live.xt = [
            Relay(f"x{d}", xb.at[d], t_send.at[0, d], t_recv.at[0, d], tp) for d in range(n_ep)
        ]
        live.ht = [
            Relay(f"h{d}", hb.at[d], t_send.at[1, d], t_recv.at[1, d], tp) for d in range(n_ep)
        ]
        live.mt = [
            Relay(
                f"m{k}", mb.at[:, pl.ds(k * half, half)], t_send.at[2, k], t_recv.at[2, k], tp
            )
            for k in range(2)
        ]

    pieces = (
        (wg_hbm, wgu.at[:, :, pl.ds(0, ffw)]),
        (wu_hbm, wgu.at[:, :, pl.ds(ffw, ffw)]),
        (wd_hbm, wd),
        (wo_hbm, wo),
    )
    local = [
        pltpu.make_async_copy(source, target, w_sem.at[k])
        for k, (source, target) in enumerate(pieces)
    ]
    def weights(k):
        if k not in live.fetched:
            live.fetched.add(k)
            with jax.named_scope(f"ww_{k}"):
                local[k].wait()

    def own_keys():
        tables(cos_ref, sin_ref, ep * length)
        kv[0, :, pl.ds(kw, kw)] = v_ref[...]
        kv[0, :, pl.ds(0, kw)] = norm_turn(
            k_ref[...],
            jnp.concatenate([kg_ref[...]] * (kw // HEAD), axis=1),
            cos_ref[:, :kw],
            sin_ref[:, :kw],
        ).astype(BF16)

    def send_keys():
        kv_copy(0).start()
        kv_copy(1).start()

    def keys_on():
        with jax.named_scope("wkv_1"):
            kv_copy(1).wait_recv()
        kv_copy(2).start()

    def keys_ready():
        with jax.named_scope("wkv_0"):
            kv_copy(0).wait_recv()
        with jax.named_scope("wkv_2"):
            kv_copy(2).wait_recv()

    def turn_queries():
        qw = cos_ref.shape[1]
        gain = jnp.concatenate([qg_ref[...]] * (qw // HEAD), axis=1)
        for i in range(q_ref.shape[1] // qw):
            part = pl.ds(i * qw, qw)
            turned = norm_turn(q_ref[:, part], gain, cos_ref[...], sin_ref[...])
            qb[:, part] = (turned.astype(BF16).astype(F32) * (1.0 / math.sqrt(HEAD))).astype(BF16)

    def x_arrived(d):
        with jax.named_scope(f"wxz_{d}"):
            x_copy(d).wait_recv()

    def hidden(d):
        total = jnp.zeros((cap, 2 * ffw), F32)
        squares = jnp.zeros((cap, 1), F32)
        for m in NEAR + FAR:
            live.xt[d].ready(m)
            weights(0)
            weights(1)
            block = xb[d, m].astype(F32)
            squares += jnp.sum(block * block, axis=1, keepdims=True)
            scaled = (block * xg_ref[tp ^ m]).astype(BF16)
            total += jnp.dot(scaled, wgu[tp ^ m], preferred_element_type=F32)
        stat = lax.rsqrt(squares / xg_ref.shape[0] / xg_ref.shape[2] + EPS)
        gate = total[:, :ffw] * stat
        up = total[:, ffw:] * stat
        hb[d, 0] = (gate / (1.0 + jnp.exp(-gate)) * up).astype(BF16)

    def down(d):
        total = jnp.zeros((ob.shape[1], ob.shape[2]), F32)
        for m in NEAR + FAR:
            live.ht[d].ready(m)
            weights(2)
            total += jnp.dot(hb[d, m], wd[tp ^ m], preferred_element_type=F32)
        ob[d] = total.astype(BF16)
        if d:
            r_copy(d).start()

    def attention(part, pair):
        keys = n_ep * length
        rows = pl.ds(part * half, half)
        outs = []
        for h in range(2 * pair, 2 * pair + 2):
            g = h * KV_HEADS // Q_HEADS
            query = qb[rows, pl.ds(h * HEAD, HEAD)]
            key = kv[:, :, pl.ds(g * HEAD, HEAD)].reshape(keys, HEAD)
            value = kv[:, :, pl.ds(kw + g * HEAD, HEAD)].reshape(keys, HEAD)
            scores = lax.dot_general(
                query, key, (((1,), (1,)), ((), ())), preferred_element_type=F32
            )
            raw = jnp.exp(scores - jnp.max(scores, axis=1, keepdims=True))
            total = jnp.sum(raw, axis=1, keepdims=True)
            out = jnp.dot(raw.astype(BF16), value, preferred_element_type=F32)
            outs.append(out / total)
        lane = pl.ds(2 * pair * HEAD, 2 * HEAD)
        mb[0, rows, lane] = jnp.concatenate(outs, axis=1).astype(BF16)

    def project(part):
        rows = pl.ds(part * half, half)
        total = jnp.zeros((half, att_ref.shape[1]), F32)
        squares = jnp.zeros((half, 1), F32)
        for m in NEAR + FAR:
            live.mt[part].ready(m)
            weights(3)
            block = mb[m, rows, :].astype(F32)
            squares += jnp.sum(block * block, axis=1, keepdims=True)
            scaled = (block * mg_ref[tp ^ m]).astype(BF16)
            total += jnp.dot(scaled, wo[tp ^ m], preferred_element_type=F32)
        scale = lax.rsqrt(squares / mg_ref.shape[0] / mg_ref.shape[2] + EPS)
        att_ref[rows, :] = (total * scale).astype(BF16)

    places = {}

    def columns():
        stack = jnp.concatenate(
            [slot_t[0].astype(F32), slot_t[1].astype(F32), rwt_ref[...]] * 2, axis=0
        )
        column = lax.dot_general(
            jnp.where(i0 == i1, 1.0, 0.0).astype(F32), stack, (((1,), (1,)), ((), ())),
            precision=lax.Precision.HIGHEST, preferred_element_type=F32,
        )
        places["slot"] = [(column[:, k : k + 1] + 0.5).astype(jnp.int32) for k in range(2)]
        places["weight"] = [column[:, 2 + k : 3 + k] for k in range(2)]

    def combine(d, first=False, last=False):
        if d:
            with jax.named_scope(f"wr_{d}"):
                r_copy(d).wait_recv()
        back = rb[d] if d else ob[0]
        index = (ep ^ d) * cap + iota((length, cap), 1)
        total = []
        for k in range(2):
            choose = jnp.where(places["slot"][k] == index, 1.0, 0.0).astype(BF16)
            found = jnp.dot(choose, back, preferred_element_type=F32)
            total.append(found if first else ct[k] + found)
        if last:
            weight = places["weight"]
            mix_ref[...] = (total[0] * weight[0] + total[1] * weight[1]).astype(BF16)
        else:
            for k in range(2):
                ct[k] = total[k]

    def step(name, f, *args, **kwargs):
        with jax.named_scope("S_" + name):
            f(*args, **kwargs)

    def send_x(d):
        xo[d] = picked_rows(d)
        x_copy(d).start()

    def finish():
        with jax.named_scope("S_drain"):
            for i, buf in enumerate((xo, rb, kv)):
                part = buf.at[pl.ds(0, n_ep - 1)]
                ep_copy(part, part, 1, z_send.at[i], z_recv.at[i, 0]).wait_send()
            for gather in live.xt + live.ht + live.mt:
                gather.drain()

    for copy in local:
        copy.start()
    xb[0, 0] = picked_rows(0)
    with jax.named_scope("S_barrier"):
        pl.semaphore_wait(barrier, n_ep + n_tp - 2)
    fresh()
    step("X0own", live.xt[0].issue, OWN)
    step("sx2", send_x, 2)
    step("sx1", send_x, 1)
    step("keys", own_keys)
    step("columns", columns)

    @pl.when(inner == 1)
    def _():
        fresh()
        step("X0fwd", live.xt[0].issue, FORWARD)
        step("X0side", live.xt[0].issue, SIDE)
        step("ax2", x_arrived, 2)
        step("X2own", live.xt[2].issue, OWN)
        step("sx3", send_x, 3)
        step("X0cor", live.xt[0].issue, CORNER)
        step("hid0", hidden, 0)
        step("X2fwd", live.xt[2].issue, FORWARD)
        step("ax1", x_arrived, 1)
        step("X1own", live.xt[1].issue, OWN)
        step("X2side", live.xt[2].issue, SIDE)
        step("X2cor", live.xt[2].issue, CORNER)
        step("X1fwd", live.xt[1].issue, FORWARD)
        step("hid2", hidden, 2)
        step("H2own", live.ht[2].issue, OWN)
        step("ax3", x_arrived, 3)
        step("sendkv", send_keys)
        step("X3lead", live.xt[3].issue, LEAD)
        step("X1side", live.xt[1].issue, SIDE)
        step("X1cor", live.xt[1].issue, CORNER)
        step("H2fwd", live.ht[2].issue, FORWARD)
        step("X3rest", live.xt[3].issue, REST)
        step("H2side", live.ht[2].issue, SIDE)
        step("queries", turn_queries)
        step("keyson", keys_on)
        step("hid1", hidden, 1)
        step("X3fwd", live.xt[3].issue, FORWARD)
        step("H1own", live.ht[1].issue, OWN)
        step("H2cor", live.ht[2].issue, CORNER)
        step("down2", down, 2)
        step("X3side", live.xt[3].issue, SIDE)
        step("wkv", keys_ready)
        step("att00", attention, 0, 0)
        step("X3cor", live.xt[3].issue, CORNER)
        step("H1fwd", live.ht[1].issue, FORWARD)
        step("hid3", hidden, 3)
        step("H3own", live.ht[3].issue, OWN)
        step("H1side", live.ht[1].issue, SIDE)
        step("att01", attention, 0, 1)
        step("M0own", live.mt[0].issue, OWN)
        step("H1cor", live.ht[1].issue, CORNER)
        step("att10", attention, 1, 0)
        step("H3fwd", live.ht[3].issue, FORWARD)
        step("H0own", live.ht[0].issue, OWN)
        step("down1", down, 1)
        step("att11", attention, 1, 1)
        step("M0fwd", live.mt[0].issue, FORWARD)
        step("M1own", live.mt[1].issue, OWN)
        step("H3side", live.ht[3].issue, SIDE)
        step("H3cor", live.ht[3].issue, CORNER)
        step("M0side", live.mt[0].issue, SIDE)
        step("down3", down, 3)
        step("H0fwd", live.ht[0].issue, FORWARD)
        step("M0cor", live.mt[0].issue, CORNER)
        step("M1fwd", live.mt[1].issue, FORWARD)
        step("H0side", live.ht[0].issue, SIDE)
        step("H0cor", live.ht[0].issue, CORNER)
        step("project0", project, 0)
        step("M1side", live.mt[1].issue, SIDE)
        step("down0", down, 0)
        step("comb0F", combine, 0, first=True)
        step("M1cor", live.mt[1].issue, CORNER)
        step("comb2", combine, 2)
        step("comb1", combine, 1)
        step("project1", project, 1)
        step("comb3L", combine, 3, last=True)
        finish()

    @pl.when(inner == 0)
    def _():
        fresh()
        step("X0fwd", live.xt[0].issue, FORWARD)
        step("X0side", live.xt[0].issue, SIDE)
        step("ax1", x_arrived, 1)
        step("X1own", live.xt[1].issue, OWN)
        step("sx3", send_x, 3)
        step("X0cor", live.xt[0].issue, CORNER)
        step("hid0", hidden, 0)
        step("X1fwd", live.xt[1].issue, FORWARD)
        step("ax2", x_arrived, 2)
        step("X2own", live.xt[2].issue, OWN)
        step("X1side", live.xt[1].issue, SIDE)
        step("X1cor", live.xt[1].issue, CORNER)
        step("X2fwd", live.xt[2].issue, FORWARD)
        step("ax3", x_arrived, 3)
        step("X3own", live.xt[3].issue, OWN)
        step("sendkv", send_keys)
        step("hid1", hidden, 1)
        step("X2side", live.xt[2].issue, SIDE)
        step("queries", turn_queries)
        step("X2cor", live.xt[2].issue, CORNER)
        step("X3fwd", live.xt[3].issue, FORWARD)
        step("hid2", hidden, 2)
        step("H2own", live.ht[2].issue, OWN)
        step("H1own", live.ht[1].issue, OWN)
        step("X3side", live.xt[3].issue, SIDE)
        step("keyson", keys_on)
        step("X3cor", live.xt[3].issue, CORNER)
        step("H2fwd", live.ht[2].issue, FORWARD)
        step("hid3", hidden, 3)
        step("H3own", live.ht[3].issue, OWN)
        step("H2side", live.ht[2].issue, SIDE)
        step("H1fwd", live.ht[1].issue, FORWARD)
        step("wkv", keys_ready)
        step("att00", attention, 0, 0)
        step("H2cor", live.ht[2].issue, CORNER)
        step("down2", down, 2)
        step("H1side", live.ht[1].issue, SIDE)
        step("H3fwd", live.ht[3].issue, FORWARD)
        step("att01", attention, 0, 1)
        step("M0own", live.mt[0].issue, OWN)
        step("H0own", live.ht[0].issue, OWN)
        step("H1cor", live.ht[1].issue, CORNER)
        step("att10", attention, 1, 0)
        step("H3side", live.ht[3].issue, SIDE)
        step("att11", attention, 1, 1)
        step("M1own", live.mt[1].issue, OWN)
        step("H3cor", live.ht[3].issue, CORNER)
        step("down3", down, 3)
        step("M0fwd", live.mt[0].issue, FORWARD)
        step("down1", down, 1)
        step("M0side", live.mt[0].issue, SIDE)
        step("H0fwd", live.ht[0].issue, FORWARD)
        step("M1fwd", live.mt[1].issue, FORWARD)
        step("M0cor", live.mt[0].issue, CORNER)
        step("H0side", live.ht[0].issue, SIDE)
        step("H0cor", live.ht[0].issue, CORNER)
        step("project0", project, 0)
        step("M1side", live.mt[1].issue, SIDE)
        step("down0", down, 0)
        step("comb0F", combine, 0, first=True)
        step("comb1", combine, 1)
        step("M1cor", live.mt[1].issue, CORNER)
        step("comb2", combine, 2)
        step("project1", project, 1)
        step("comb3L", combine, 3, last=True)
        finish()


def hand_on(a_ref, b_ref, a_out, b_out, sems):
    copies = [
        pltpu.make_async_copy(a_ref, a_out, sems.at[0]),
        pltpu.make_async_copy(b_ref, b_out, sems.at[1]),
    ]
    for copy in copies:
        copy.start()
    for copy in copies:
        copy.wait()


def hand_out(outs):
    return pl.pallas_call(
        hand_on,
        out_shape=tuple(jax.ShapeDtypeStruct(o.shape, o.dtype) for o in outs),
        in_specs=[pl.BlockSpec(memory_space=pltpu.VMEM)] * 2,
        out_specs=[pl.BlockSpec(memory_space=pl.ANY)] * 2,
        scratch_shapes=[pltpu.SemaphoreType.DMA((2,))],
    )(*(pltpu.with_memory_space_constraint(o, pltpu.VMEM) for o in outs))


def shards(
    n_ep, n_tp,
    queries, key_rows, values, query_gain, key_gain, mix_gain, out_weight, expert_input,
    expert_gain, route_ids, route_weights, expert_gate, expert_up, expert_down,
):
    length, width = expert_input.shape
    qw, kw = queries.shape[1], key_rows.shape[1]
    ffw = expert_gate.shape[2]
    out_w = out_weight.shape[1]
    copies = length * route_ids.shape[1]
    capacity = (4 * copies + 3 * n_ep - 1) // (3 * n_ep)
    cap = (capacity + 15) // 16 * 16
    groups = 4
    rows = cap * (n_ep // groups)
    plan = gather_plan(n_tp)

    table_w = min(128, qw)
    operands = (
        queries, key_rows, values,
        query_gain.reshape(1, HEAD), key_gain.reshape(1, HEAD),
        mix_gain.reshape(n_tp, 1, qw),
        out_weight.reshape(n_tp, qw, out_w),
        expert_input,
        expert_gain.reshape(n_tp, 1, width),
        route_ids.T, route_weights.T,
        expert_gate.reshape(n_tp, width, ffw),
        expert_up.reshape(n_tp, width, ffw),
        expert_down.reshape(n_tp, ffw, out_w),
    )
    vmem = pl.BlockSpec(memory_space=pltpu.VMEM)
    hbm = pl.BlockSpec(memory_space=pl.ANY)
    specs = [hbm if i in (6, 11, 12, 13) else vmem for i in range(len(operands))]
    dma = pltpu.SemaphoreType.DMA
    line = n_ep == 4 and n_tp == 8
    tables_at = [pltpu.VMEM((length, table_w), F32)] * 2
    blocks_at = [
        pltpu.VMEM((n_ep, cap, width), BF16),
        pltpu.VMEM((groups, n_tp, rows, width), BF16),
        pltpu.VMEM((groups, n_tp, rows, ffw), BF16),
        pltpu.VMEM((n_tp, length, qw), BF16),
    ]
    weights_at = [
        pltpu.VMEM((n_tp, width, 2 * ffw), BF16),
        pltpu.VMEM((n_tp, ffw, out_w), BF16),
        pltpu.VMEM((n_tp, qw, out_w), BF16),
    ]
    results_at = [
        pltpu.VMEM((length, qw), BF16),
        pltpu.VMEM((groups, rows, out_w), BF16),
        pltpu.VMEM((n_ep, cap, out_w), BF16),
    ]
    if line:
        body = functools.partial(line_kernel, n_ep, n_tp, cap)
        scratch = tables_at + blocks_at + [pltpu.VMEM((n_ep, length, 2 * kw), BF16)]
        scratch += results_at + [pltpu.VMEM((2, length, out_w), F32)] + weights_at
        scratch += [dma((4,)), dma((3,)), dma((3, n_ep)), dma((3, n_ep)), dma((3, n_ep, 4))]
    else:
        body = functools.partial(kernel, n_ep, n_tp, cap, plan)
        scratch = tables_at + blocks_at + [pltpu.VMEM((n_ep, length, kw), BF16)] * 2
        scratch += results_at + weights_at
        scratch += [dma((4, n_tp)), dma((1,))] + [dma((n_ep,))] * 8
        scratch += [dma((groups, len(plan)))] * 4 + [dma((len(plan),))] * 2
    outs = pl.pallas_call(
        body,
        out_shape=(
            pltpu.VMEM((length, out_w), BF16),
            pltpu.VMEM((length, out_w), BF16),
        ),
        in_specs=specs,
        out_specs=(vmem, vmem),
        scratch_shapes=scratch,
        compiler_params=pltpu.CompilerParams(
            collective_id=0, has_side_effects=True, vmem_limit_bytes=60 * 1024 * 1024
        ),
    )(*operands)
    return hand_out(outs)


def solution(mesh):
    placed = (
        P("ep", "tp"), P("ep", "tp"), P("ep", "tp"), P(), P(), P(), P(None, "tp"),
        P("ep", "tp"), P(), P("ep", None), P("ep", None),
        P("ep", None, "tp"), P("ep", None, "tp"), P("ep", None, "tp"),
    )
    return jax.shard_map(
        functools.partial(shards, mesh.shape["ep"], mesh.shape["tp"]),
        mesh=mesh,
        in_specs=placed,
        out_specs=(P("ep", "tp"), P("ep", "tp")),
        check_vma=False,
    )
```

```python
import functools
import math
import types

import jax
import jax.numpy as jnp
import numpy as np
from jax import lax
from jax.experimental import pallas as pl
from jax.experimental.pallas import tpu as pltpu
from jax.sharding import PartitionSpec as P

Q_HEADS = 32
KV_HEADS = 16
HEAD = 64
GRID_W = 64
EPS = 1e-06
THETA = 10000.0
MESH = pl.DeviceIdType.MESH
F32 = jnp.float32
BF16 = jnp.bfloat16


def gather_plan(n_tp):
    if n_tp == 8:
        return (
            (2, 0, None, None),
            (4, 0, None, None),
            (1, 0, None, None),
            (4, 2, 0, 0),
            (2, 4, 1, 1),
            (1, 2, None, 0),
            (1, 4, None, 1),
            (1, 6, 0, 3),
            (1, 6, 1, 4),
        )
    return tuple((m, 0, None, None) for m in range(1, n_tp))


def plan_stages(plan):
    depth = []
    for entry in plan:
        depth.append(0 if entry[3] is None else depth[entry[3]] + 1)
    return [[i for i, d in enumerate(depth) if d == k] for k in range(3)]


class Gather:
    def __init__(self, name, plan, buf, send, recv, tp):
        self.name = name
        self.plan, self.buf, self.send, self.recv, self.tp = plan, buf, send, recv, tp
        self.stages = plan_stages(plan)
        self.waited = set()
        self.sent = []

    def part(self, block, half):
        if half is None:
            return self.buf.at[block]
        width = self.buf.shape[-1] // 2
        return self.buf.at[block, :, pl.ds(half * width, width)]

    def copy(self, i):
        target, block, half, _ = self.plan[i]
        return pltpu.make_async_remote_copy(
            src_ref=self.part(block, half),
            dst_ref=self.part(block ^ target, half),
            send_sem=self.send.at[i],
            recv_sem=self.recv.at[i],
            device_id={"tp": self.tp ^ target},
            device_id_type=MESH,
        )

    def wait_entry(self, i):
        if i not in self.waited:
            self.waited.add(i)
            with jax.named_scope(f"w{self.name}_{i}"):
                self.copy(i).wait_recv()

    def stage(self, k):
        for i in self.stages[k]:
            if self.plan[i][3] is not None:
                self.wait_entry(self.plan[i][3])
            copy = self.copy(i)
            copy.start()
            self.sent.append(copy)

    def ready(self, block):
        for i, entry in enumerate(self.plan):
            if entry[1] ^ entry[0] == block:
                self.wait_entry(i)

    def order(self):
        blocks = [0]
        for entry in self.plan:
            if entry[0] ^ entry[1] not in blocks:
                blocks.append(entry[0] ^ entry[1])
        return blocks

    def drain(self):
        for copy in self.sent:
            copy.wait_send()


def iota(shape, axis):
    return lax.broadcasted_iota(jnp.int32, shape, axis)


def exact_dot(a, b):
    return jnp.dot(a, b, precision=lax.Precision.HIGHEST, preferred_element_type=F32)


def norm_turn(source, gain, cosine, sine):
    width = source.shape[1]
    rows = source.astype(F32)
    i0, i1 = iota((width, width), 0), iota((width, width), 1)
    same_head = jnp.where(i0 // HEAD == i1 // HEAD, 1.0 / HEAD, 0.0).astype(F32)
    mean = exact_dot(rows * rows, same_head)
    rows = rows * lax.rsqrt(mean + EPS) * gain
    partner = jnp.where(i1 % 2 == 0, i1 + 1, i1 - 1)
    sign = jnp.where(i1 % 2 == 0, -1.0, 1.0)
    swap = jnp.where(i0 == partner, sign, 0.0).astype(F32)
    return rows * cosine + exact_dot(rows, swap) * sine


def tables(cos_ref, sin_ref, offset):
    length, width = cos_ref.shape
    half_width = HEAD // 2
    inverse = THETA ** (-np.arange(0, half_width, 2, dtype=np.float32) / half_width)
    pair = iota((1, width), 1) % HEAD // 2
    row_inv = jnp.zeros((1, width), F32)
    for m, value in enumerate(inverse.astype(np.float32)):
        row_inv = jnp.where(pair % len(inverse) == m, float(value), row_inv)
    position = offset + iota((length, width), 0)
    grid = jnp.where(
        iota((length, width), 1) % HEAD < half_width, position // GRID_W, position % GRID_W
    ).astype(F32)
    angle = grid * row_inv
    cos_ref[...] = jnp.cos(angle)
    sin_ref[...] = jnp.sin(angle)


def kernel(
    n_ep, n_tp, cap, plan,
    q_ref, k_ref, v_ref, qg_ref, kg_ref, mg_ref, wo_hbm, x_ref, xg_ref,
    idst_ref, rwt_ref, wg_hbm, wu_hbm, wd_hbm,
    att_ref, mix_ref,
    cos_ref, sin_ref, xo, xb, hb, mb, kb, vb, qb, ob, rb, wgu, wd, wo,
    w_sem, v_sem,
    xz_send, xz_recv, kz_send, kz_recv, vz_send, vz_recv, rz_send, rz_recv,
    xt_send, xt_recv, ht_send, ht_recv, mt_send, mt_recv,
):
    ep, tp = lax.axis_index("ep"), lax.axis_index("tp")
    groups = xb.shape[0]
    per = n_ep // groups
    length = x_ref.shape[0]
    ffw = hb.shape[-1]

    barrier = pltpu.get_barrier_semaphore()
    for d in range(1, n_ep):
        pl.semaphore_signal(barrier, inc=1, device_id={"ep": ep ^ d}, device_id_type=MESH)
    for m in range(1, n_tp):
        pl.semaphore_signal(barrier, inc=1, device_id={"tp": tp ^ m}, device_id_type=MESH)

    lanes = (n_ep + 15) // 16 * 16
    hit_t = [(idst_ref[k : k + 1, :] == iota((lanes, length), 0)) for k in range(2)]
    both_t = sum(jnp.where(h, 1.0, 0.0) for h in hit_t).astype(BF16)
    i0, i1 = iota((length, length), 0), iota((length, length), 1)
    before_t = jnp.where(i0 < i1, 1.0, 0.0).astype(BF16)
    count_t = jnp.dot(both_t, before_t, preferred_element_type=F32)
    slot_t = [
        jnp.sum(jnp.where(hit_t[k], count_t, 0.0), axis=0, keepdims=True).astype(jnp.int32)
        + idst_ref[k : k + 1, :] * cap
        for k in range(2)
    ]

    def picked_rows(d):
        index = (ep ^ d) * cap + iota((cap, length), 0)
        choose = jnp.where((slot_t[0] == index) | (slot_t[1] == index), 1.0, 0.0).astype(BF16)
        return jnp.dot(choose, x_ref[...], preferred_element_type=F32).astype(BF16)

    sends = []

    def ep_copy(source, target, d, send, recv):
        return pltpu.make_async_remote_copy(
            src_ref=source, dst_ref=target, send_sem=send.at[d], recv_sem=recv.at[d],
            device_id={"ep": ep ^ d}, device_id_type=MESH,
        )

    def x_copy(d):
        return ep_copy(
            xo.at[d], xb.at[d // per, 0, pl.ds((d % per) * cap, cap)], d, xz_send, xz_recv
        )

    xt = [Gather(f"x{c}", plan, xb.at[c], xt_send.at[c], xt_recv.at[c], tp) for c in range(groups)]
    ht = [Gather(f"h{c}", plan, hb.at[c], ht_send.at[c], ht_recv.at[c], tp) for c in range(groups)]
    mt = Gather("m", plan, mb, mt_send, mt_recv, tp)

    xb[0, 0, pl.ds(0, cap), :] = picked_rows(0)
    pl.semaphore_wait(barrier, n_ep + n_tp - 2)
    if per == 1:
        xt[0].stage(0)

    def send_rows(c):
        for d in range(c * per, (c + 1) * per):
            if d:
                copy = x_copy(d)
                copy.start()
                sends.append(copy)

    for d in range(1, n_ep):
        xo[d] = picked_rows(d)
        if d == max(per - 1, 1):
            for c in range(0 if per > 1 else 1, 1 if per > 1 else 2):
                send_rows(c)

    def x_first(c):
        for d in range(c * per, (c + 1) * per):
            if d:
                x_copy(d).wait_recv()
        xt[c].stage(0)

    local = []
    for m in range(n_tp):
        p = tp ^ m
        pieces = (
            (wg_hbm.at[p], wgu.at[m, :, pl.ds(0, ffw)]),
            (wu_hbm.at[p], wgu.at[m, :, pl.ds(ffw, ffw)]),
            (wd_hbm.at[p], wd.at[m]),
            (wo_hbm.at[p], wo.at[m]),
        )
        for k, (source, target) in enumerate(pieces):
            copy = pltpu.make_async_copy(source, target, w_sem.at[k, m])
            copy.start()
            local.append(((k, m), copy))
    local = dict(local)
    own_v = pltpu.make_async_copy(v_ref, vb.at[0], v_sem.at[0])
    own_v.start()

    if per > 1:
        x_first(0)

    tables(cos_ref, sin_ref, ep * length)
    kb[0] = norm_turn(
        k_ref[...],
        jnp.concatenate([kg_ref[...]] * (k_ref.shape[1] // HEAD), axis=1),
        cos_ref[:, : k_ref.shape[1]],
        sin_ref[:, : k_ref.shape[1]],
    ).astype(BF16)
    own_v.wait()

    def send_keys():
        for d in range(1, n_ep):
            for source, target, send, recv in (
                (kb.at[0], kb.at[d], kz_send, kz_recv),
                (vb.at[0], vb.at[d], vz_send, vz_recv),
            ):
                copy = ep_copy(source, target, d, send, recv)
                copy.start()
                sends.append(copy)

    def turn_queries():
        qw = cos_ref.shape[1]
        gain = jnp.concatenate([qg_ref[...]] * (qw // HEAD), axis=1)
        for i in range(q_ref.shape[1] // qw):
            part = pl.ds(i * qw, qw)
            turned = norm_turn(q_ref[:, part], gain, cos_ref[...], sin_ref[...])
            qb[:, part] = (turned.astype(BF16).astype(F32) * (1.0 / math.sqrt(HEAD))).astype(BF16)

    fetched = set()

    def weights(k, m):
        if (k, m) not in fetched:
            fetched.add((k, m))
            local[k, m].wait()

    def hidden(c):
        rows = xb.shape[2]
        total = jnp.zeros((rows, 2 * ffw), F32)
        squares = jnp.zeros((rows, 1), F32)
        for m in xt[c].order():
            xt[c].ready(m)
            weights(0, m)
            weights(1, m)
            block = xb[c, m].astype(F32)
            squares += jnp.sum(block * block, axis=1, keepdims=True)
            scaled = (block * xg_ref[tp ^ m]).astype(BF16)
            total += jnp.dot(scaled, wgu[m], preferred_element_type=F32)
        stat = lax.rsqrt(squares / xg_ref.shape[0] / xg_ref.shape[2] + EPS)
        gate = total[:, :ffw] * stat
        up = total[:, ffw:] * stat
        hb[c, 0] = (gate / (1.0 + jnp.exp(-gate)) * up).astype(BF16)

    def r_copy(d):
        return ep_copy(
            ob.at[d // per, pl.ds((d % per) * cap, cap)], rb.at[d], d, rz_send, rz_recv
        )

    def down(c):
        total = jnp.zeros((ob.shape[1], ob.shape[2]), F32)
        for m in ht[c].order():
            ht[c].ready(m)
            weights(2, m)
            total += jnp.dot(hb[c, m], wd[m], preferred_element_type=F32)
        ob[c] = total.astype(BF16)
        for d in range(c * per, (c + 1) * per):
            if d:
                copy = r_copy(d)
                copy.start()
                sends.append(copy)

    def keys_ready():
        for d in range(1, n_ep):
            ep_copy(kb.at[0], kb.at[d], d, kz_send, kz_recv).wait_recv()
            ep_copy(vb.at[0], vb.at[d], d, vz_send, vz_recv).wait_recv()

    def attention(part):
        keys = n_ep * length
        block = length // 2
        rows = pl.ds(part * block, block)
        outs = []
        for h in range(q_ref.shape[1] // HEAD):
            g = h * KV_HEADS // Q_HEADS
            lane = pl.ds(g * HEAD, HEAD)
            query = qb[rows, pl.ds(h * HEAD, HEAD)]
            key = kb[:, :, lane].reshape(keys, HEAD)
            value = vb[:, :, lane].reshape(keys, HEAD)
            scores = lax.dot_general(
                query, key, (((1,), (1,)), ((), ())), preferred_element_type=F32
            )
            raw = jnp.exp(scores - jnp.max(scores, axis=1, keepdims=True))
            total = jnp.sum(raw, axis=1, keepdims=True)
            out = jnp.dot(raw.astype(BF16), value, preferred_element_type=F32)
            outs.append(out / total)
        mb[0, rows, :] = jnp.concatenate(outs, axis=1).astype(BF16)

    def project():
        total = jnp.zeros(att_ref.shape, F32)
        squares = jnp.zeros((length, 1), F32)
        for m in mt.order():
            mt.ready(m)
            weights(3, m)
            block = mb[m].astype(F32)
            squares += jnp.sum(block * block, axis=1, keepdims=True)
            scaled = (block * mg_ref[tp ^ m]).astype(BF16)
            total += jnp.dot(scaled, wo[m], preferred_element_type=F32)
        scale = lax.rsqrt(squares / mg_ref.shape[0] / mg_ref.shape[2] + EPS)
        att_ref[...] = (total * scale).astype(BF16)

    def combine():
        stack = jnp.concatenate(
            [slot_t[0].astype(F32), slot_t[1].astype(F32), rwt_ref[...]] * 2, axis=0
        )
        columns = lax.dot_general(
            jnp.where(i0 == i1, 1.0, 0.0).astype(F32), stack, (((1,), (1,)), ((), ())),
            precision=lax.Precision.HIGHEST, preferred_element_type=F32,
        )
        slot = [(columns[:, k : k + 1] + 0.5).astype(jnp.int32) for k in range(2)]
        total = [jnp.zeros(mix_ref.shape, F32) for k in range(2)]
        for d in range(n_ep):
            if d:
                r_copy(d).wait_recv()
                back = rb[d]
            else:
                back = ob[0, pl.ds(0, cap), :]
            index = (ep ^ d) * cap + iota((length, cap), 1)
            for k in range(2):
                choose = jnp.where(slot[k] == index, 1.0, 0.0).astype(BF16)
                total[k] += jnp.dot(choose, back, preferred_element_type=F32)
        mix_ref[...] = (total[0] * columns[:, 2:3] + total[1] * columns[:, 3:4]).astype(BF16)


    if per > 1:
        send_rows(1)
    send_rows(2)
    xt[0].stage(1)
    x_first(1)
    send_rows(3)
    xt[0].stage(2)
    turn_queries()
    hidden(0)
    ht[0].stage(0)
    xt[1].stage(1)
    ht[0].stage(1)
    xt[1].stage(2)
    x_first(2)
    send_keys()
    hidden(1)
    ht[1].stage(0)
    ht[0].stage(2)
    xt[2].stage(1)
    x_first(3)
    down(0)
    ht[1].stage(1)
    xt[2].stage(2)
    hidden(2)
    ht[2].stage(0)
    xt[3].stage(1)
    ht[1].stage(2)
    down(1)
    ht[2].stage(1)
    keys_ready()
    attention(0)
    xt[3].stage(2)
    ht[2].stage(2)
    hidden(3)
    ht[3].stage(0)
    down(2)
    attention(1)
    ht[3].stage(1)
    mt.stage(0)
    ht[3].stage(2)
    down(3)
    mt.stage(1)
    mt.stage(2)
    project()
    combine()

    for copy in sends:
        copy.wait_send()
    for gather in xt + ht + [mt]:
        gather.drain()


RELAY_PLAN = (
    (2, 0, 0),
    (4, 0, 1),
    (2, 0, 1),
    (4, 0, 0),
    (4, 2, 0),
    (2, 4, 1),
    (1, 0, None),
    (1, 2, None),
    (1, 4, None),
    (1, 6, None),
)
RELAY_WAIT = (0, 0, 1, 1, 2, 2, 3, 3, 3, 3)
OWN = (0, 1, 2, 3, 6)
LEAD = (0, 1)
REST = (2, 3, 6)
FORWARD = (4, 5)
SIDE = (7, 8)
CORNER = (9,)
NEEDS = {FORWARD: 0, SIDE: 1, CORNER: 2}
NEAR = (0, 2, 4, 6)
FAR = (1, 3, 5, 7)
FIRST = NEAR[:3]
SECOND = NEAR[3:] + FAR


class Relay:
    def __init__(self, name, buf, send, recv, tp):
        self.name = name
        self.buf, self.send, self.recv, self.tp = buf, send, recv, tp
        self.waited = set()

    def part(self, block, half):
        if half is None:
            return self.buf.at[block]
        width = self.buf.shape[-1] // 2
        return self.buf.at[block, :, pl.ds(half * width, width)]

    def copy(self, i):
        target, block, half = RELAY_PLAN[i]
        return pltpu.make_async_remote_copy(
            src_ref=self.part(block, half),
            dst_ref=self.part(block ^ target, half),
            send_sem=self.send,
            recv_sem=self.recv.at[RELAY_WAIT[i]],
            device_id={"tp": self.tp ^ target},
            device_id_type=MESH,
        )

    def whole(self, blocks, i):
        part = self.buf.at[pl.ds(0, blocks)]
        return pltpu.make_async_remote_copy(
            src_ref=part, dst_ref=part, send_sem=self.send, recv_sem=self.recv.at[i],
            device_id={"tp": self.tp ^ 1}, device_id_type=MESH,
        )

    def wait(self, i):
        if i not in self.waited:
            self.waited.add(i)
            with jax.named_scope(f"w{self.name}_{i}"):
                self.whole(len(FAR) if i == 3 else 1, i).wait_recv()

    def issue(self, entries):
        if entries in NEEDS:
            self.wait(NEEDS[entries])
        for i in entries:
            self.copy(i).start()

    def ready(self, block):
        if block in FAR:
            self.wait(3)
        elif block:
            for i in (0, 1, 2) if block in SECOND else (0, 1):
                self.wait(i)


def line_kernel(
    n_ep, n_tp, cap,
    q_ref, k_ref, v_ref, qg_ref, kg_ref, mg_ref, wo_hbm, x_ref, xg_ref,
    idst_ref, rwt_ref, wg_hbm, wu_hbm, wd_hbm,
    att_ref, mix_ref,
    cos_ref, sin_ref, xo, xb, hb, mb, kv, qb, ob, rb, ct, wgu, wd, wo,
    w_sem, z_send, z_recv, t_send, t_recv,
):
    ep, tp = lax.axis_index("ep"), lax.axis_index("tp")
    length = x_ref.shape[0]
    ffw = hb.shape[-1]
    kw = k_ref.shape[1]
    half = length // 2
    inner = (ep + 1) // 2 % 2

    barrier = pltpu.get_barrier_semaphore()
    for d in range(1, n_ep):
        pl.semaphore_signal(barrier, inc=1, device_id={"ep": ep ^ d}, device_id_type=MESH)
    for m in range(1, n_tp):
        pl.semaphore_signal(barrier, inc=1, device_id={"tp": tp ^ m}, device_id_type=MESH)

    lanes = (n_ep + 15) // 16 * 16
    hit_t = [(idst_ref[k : k + 1, :] == iota((lanes, length), 0)) for k in range(2)]
    both_t = sum(jnp.where(h, 1.0, 0.0) for h in hit_t).astype(BF16)
    i0, i1 = iota((length, length), 0), iota((length, length), 1)
    before_t = jnp.where(i0 < i1, 1.0, 0.0).astype(BF16)
    count_t = jnp.dot(both_t, before_t, preferred_element_type=F32)
    slot_t = [
        jnp.sum(jnp.where(hit_t[k], count_t, 0.0), axis=0, keepdims=True).astype(jnp.int32)
        + idst_ref[k : k + 1, :] * cap
        for k in range(2)
    ]

    def picked_rows(d):
        index = (ep ^ d) * cap + iota((cap, length), 0)
        choose = jnp.where((slot_t[0] == index) | (slot_t[1] == index), 1.0, 0.0).astype(BF16)
        return jnp.dot(choose, x_ref[...], preferred_element_type=F32).astype(BF16)

    def ep_copy(source, target, d, send, recv):
        return pltpu.make_async_remote_copy(
            src_ref=source, dst_ref=target, send_sem=send, recv_sem=recv,
            device_id={"ep": ep ^ d}, device_id_type=MESH,
        )

    def x_copy(d):
        return ep_copy(xo.at[d], xb.at[d, 0], d, z_send.at[0], z_recv.at[0, d - 1])

    def r_copy(d):
        return ep_copy(ob.at[d], rb.at[d], d, z_send.at[1], z_recv.at[1, d - 1])

    def kv_copy(i):
        d, block = ((1, 0), (2, 0), (1, 2))[i]
        return ep_copy(kv.at[block], kv.at[block ^ d], d, z_send.at[2], z_recv.at[2, i])

    live = types.SimpleNamespace()

    def fresh():
        live.fetched = set()
        live.partial = {}
        live.xt = [
            Relay(f"x{d}", xb.at[d], t_send.at[0], t_recv.at[d], tp) for d in range(n_ep)
        ]
        live.ht = [
            Relay(f"h{d}", hb.at[d], t_send.at[1], t_recv.at[n_ep + d], tp) for d in range(n_ep)
        ]
        live.mt = [
            Relay(
                f"m{k}", mb.at[:, pl.ds(k * half, half)],
                t_send.at[2], t_recv.at[2 * n_ep + k], tp,
            )
            for k in range(2)
        ]

    pieces = (
        (wg_hbm, wgu.at[:, :, pl.ds(0, ffw)]),
        (wu_hbm, wgu.at[:, :, pl.ds(ffw, ffw)]),
        (wd_hbm, wd),
        (wo_hbm, wo),
    )
    local = [
        pltpu.make_async_copy(source, target, w_sem.at[k])
        for k, (source, target) in enumerate(pieces)
    ]
    def weights(k):
        if k not in live.fetched:
            live.fetched.add(k)
            with jax.named_scope(f"ww_{k}"):
                local[k].wait()

    def own_keys():
        tables(cos_ref, sin_ref, ep * length)
        kv[0, :, pl.ds(kw, kw)] = v_ref[...]
        kv[0, :, pl.ds(0, kw)] = norm_turn(
            k_ref[...],
            jnp.concatenate([kg_ref[...]] * (kw // HEAD), axis=1),
            cos_ref[:, :kw],
            sin_ref[:, :kw],
        ).astype(BF16)

    def send_keys():
        kv_copy(0).start()
        kv_copy(1).start()

    def keys_on():
        with jax.named_scope("wkv_1"):
            kv_copy(1).wait_recv()
        kv_copy(2).start()

    def keys_ready():
        with jax.named_scope("wkv_0"):
            kv_copy(0).wait_recv()
        with jax.named_scope("wkv_2"):
            kv_copy(2).wait_recv()

    def turn_queries():
        qw = cos_ref.shape[1]
        gain = jnp.concatenate([qg_ref[...]] * (qw // HEAD), axis=1)
        for i in range(q_ref.shape[1] // qw):
            part = pl.ds(i * qw, qw)
            turned = norm_turn(q_ref[:, part], gain, cos_ref[...], sin_ref[...])
            qb[:, part] = (turned.astype(BF16).astype(F32) * (1.0 / math.sqrt(HEAD))).astype(BF16)

    def x_arrived(d):
        with jax.named_scope(f"wxz_{d}"):
            x_copy(d).wait_recv()

    def hidden(d, blocks=NEAR + FAR, last=True):
        total, squares = live.partial.pop(("x", d), (None, None))
        for m in blocks:
            live.xt[d].ready(m)
            weights(0)
            weights(1)
            block = xb[d, m].astype(F32)
            square = jnp.sum(block * block, axis=1, keepdims=True)
            scaled = (block * xg_ref[tp ^ m]).astype(BF16)
            product = jnp.dot(scaled, wgu[tp ^ m], preferred_element_type=F32)
            total = product if total is None else total + product
            squares = square if squares is None else squares + square
        if not last:
            live.partial["x", d] = total, squares
            return
        stat = lax.rsqrt(squares / xg_ref.shape[0] / xg_ref.shape[2] + EPS)
        gate = total[:, :ffw] * stat
        up = total[:, ffw:] * stat
        hb[d, 0] = (gate / (1.0 + jnp.exp(-gate)) * up).astype(BF16)

    def down(d, blocks=NEAR + FAR, last=True):
        total = live.partial.pop(("h", d), None)
        for m in blocks:
            live.ht[d].ready(m)
            weights(2)
            product = jnp.dot(hb[d, m], wd[tp ^ m], preferred_element_type=F32)
            total = product if total is None else total + product
        if not last:
            live.partial["h", d] = total
            return
        ob[d] = total.astype(BF16)
        if d:
            r_copy(d).start()

    def attention(part, pair):
        keys = n_ep * length
        rows = pl.ds(part * half, half)
        outs = []
        for h in range(2 * pair, 2 * pair + 2):
            g = h * KV_HEADS // Q_HEADS
            query = qb[rows, pl.ds(h * HEAD, HEAD)]
            key = kv[:, :, pl.ds(g * HEAD, HEAD)].reshape(keys, HEAD)
            value = kv[:, :, pl.ds(kw + g * HEAD, HEAD)].reshape(keys, HEAD)
            scores = lax.dot_general(
                query, key, (((1,), (1,)), ((), ())), preferred_element_type=F32
            )
            raw = jnp.exp(scores - jnp.max(scores, axis=1, keepdims=True))
            total = jnp.sum(raw, axis=1, keepdims=True)
            out = jnp.dot(raw.astype(BF16), value, preferred_element_type=F32)
            outs.append(out / total)
        lane = pl.ds(2 * pair * HEAD, 2 * HEAD)
        mb[0, rows, lane] = jnp.concatenate(outs, axis=1).astype(BF16)

    def project(part):
        rows = pl.ds(part * half, half)
        total = jnp.zeros((half, att_ref.shape[1]), F32)
        squares = jnp.zeros((half, 1), F32)
        for m in NEAR + FAR:
            live.mt[part].ready(m)
            weights(3)
            block = mb[m, rows, :].astype(F32)
            squares += jnp.sum(block * block, axis=1, keepdims=True)
            scaled = (block * mg_ref[tp ^ m]).astype(BF16)
            total += jnp.dot(scaled, wo[tp ^ m], preferred_element_type=F32)
        scale = lax.rsqrt(squares / mg_ref.shape[0] / mg_ref.shape[2] + EPS)
        att_ref[rows, :] = (total * scale).astype(BF16)

    places = {}

    def columns():
        stack = jnp.concatenate(
            [slot_t[0].astype(F32), slot_t[1].astype(F32), rwt_ref[...]] * 2, axis=0
        )
        column = lax.dot_general(
            jnp.where(i0 == i1, 1.0, 0.0).astype(F32), stack, (((1,), (1,)), ((), ())),
            precision=lax.Precision.HIGHEST, preferred_element_type=F32,
        )
        places["slot"] = [(column[:, k : k + 1] + 0.5).astype(jnp.int32) for k in range(2)]
        places["weight"] = [column[:, 2 + k : 3 + k] for k in range(2)]

    def combine(d, first=False, last=False):
        if d:
            with jax.named_scope(f"wr_{d}"):
                r_copy(d).wait_recv()
        back = rb[d] if d else ob[0]
        index = (ep ^ d) * cap + iota((length, cap), 1)
        total = []
        for k in range(2):
            choose = jnp.where(places["slot"][k] == index, 1.0, 0.0).astype(BF16)
            found = jnp.dot(choose, back, preferred_element_type=F32)
            total.append(found if first else ct[k] + found)
        if last:
            weight = places["weight"]
            mix_ref[...] = (total[0] * weight[0] + total[1] * weight[1]).astype(BF16)
        else:
            for k in range(2):
                ct[k] = total[k]

    def step(name, f, *args, **kwargs):
        with jax.named_scope("S_" + name):
            f(*args, **kwargs)

    def on_core(core, name, f, *args):
        @pl.when(tp % 2 == core)
        def _():
            step(name, f, *args)

    def pick_x(d):
        xo[d] = picked_rows(d)

    def send_x(d):
        if d == 3:
            pick_x(d)
        x_copy(d).start()

    def finish():
        with jax.named_scope("S_drain"):
            for i, buf in enumerate((xo, rb, kv)):
                part = buf.at[pl.ds(0, n_ep - 1)]
                ep_copy(part, part, 1, z_send.at[i], z_recv.at[i, 0]).wait_send()
            sent = pl.ds(0, n_tp - 1)
            for i, part in enumerate((xb.at[:, sent], hb.at[:, sent], mb.at[sent])):
                pltpu.make_async_remote_copy(
                    src_ref=part, dst_ref=part, send_sem=t_send.at[i], recv_sem=t_recv.at[0, 0],
                    device_id={"tp": tp ^ 1}, device_id_type=MESH,
                ).wait_send()

    for copy in local:
        copy.start()
    xb[0, 0] = picked_rows(0)
    pick_x(2)
    pick_x(1)
    with jax.named_scope("S_barrier"):
        pl.semaphore_wait(barrier, n_ep + n_tp - 2)
    fresh()
    step("sx2", send_x, 2)
    step("sx1", send_x, 1)
    step("X0lead", live.xt[0].issue, LEAD)
    step("keys", own_keys)
    step("X0rest", live.xt[0].issue, REST)
    step("columns", columns)

    @pl.when(inner == 1)
    def _():
        fresh()
        step("X0fwd", live.xt[0].issue, FORWARD)
        step("X0side", live.xt[0].issue, SIDE)
        step("ax2", x_arrived, 2)
        step("X2own", live.xt[2].issue, OWN)
        step("sx3", send_x, 3)
        step("X0cor", live.xt[0].issue, CORNER)
        step("hid0", hidden, 0)
        step("X2fwd", live.xt[2].issue, FORWARD)
        step("ax1", x_arrived, 1)
        step("X1own", live.xt[1].issue, OWN)
        step("X2side", live.xt[2].issue, SIDE)
        step("X2cor", live.xt[2].issue, CORNER)
        step("X1fwd", live.xt[1].issue, FORWARD)
        step("hid2", hidden, 2)
        step("H2own", live.ht[2].issue, OWN)
        step("ax3", x_arrived, 3)
        step("sendkv", send_keys)
        step("X3lead", live.xt[3].issue, LEAD)
        step("X1side", live.xt[1].issue, SIDE)
        step("X1cor", live.xt[1].issue, CORNER)
        step("H2fwd", live.ht[2].issue, FORWARD)
        step("X3rest", live.xt[3].issue, REST)
        step("H2side", live.ht[2].issue, SIDE)
        step("queries", turn_queries)
        step("keyson", keys_on)
        step("hid1", hidden, 1)
        step("X3fwd", live.xt[3].issue, FORWARD)
        step("H1own", live.ht[1].issue, OWN)
        step("H2cor", live.ht[2].issue, CORNER)
        step("down2", down, 2)
        step("X3side", live.xt[3].issue, SIDE)
        step("wkv", keys_ready)
        step("att00", attention, 0, 0)
        step("X3cor", live.xt[3].issue, CORNER)
        step("H1fwd", live.ht[1].issue, FORWARD)
        step("hid3", hidden, 3)
        step("H3own", live.ht[3].issue, OWN)
        step("H1side", live.ht[1].issue, SIDE)
        step("att01", attention, 0, 1)
        on_core(0, "M0own", live.mt[0].issue, OWN)
        step("H1cor", live.ht[1].issue, CORNER)
        step("att10", attention, 1, 0)
        on_core(1, "M0own", live.mt[0].issue, OWN)
        step("H3fwd", live.ht[3].issue, FORWARD)
        step("down1", down, 1)
        step("att11", attention, 1, 1)
        step("H0own", live.ht[0].issue, OWN)
        step("M0fwd", live.mt[0].issue, FORWARD)
        step("M1own", live.mt[1].issue, OWN)
        step("H3side", live.ht[3].issue, SIDE)
        step("downa3", down, 3, FIRST, False)
        step("H3cor", live.ht[3].issue, CORNER)
        step("M0side", live.mt[0].issue, SIDE)
        step("downb3", down, 3, SECOND)
        step("comb2F", combine, 2, first=True)
        step("H0fwd", live.ht[0].issue, FORWARD)
        step("M0cor", live.mt[0].issue, CORNER)
        step("M1fwd", live.mt[1].issue, FORWARD)
        step("H0side", live.ht[0].issue, SIDE)
        step("downa0", down, 0, FIRST, False)
        step("H0cor", live.ht[0].issue, CORNER)
        step("M1side", live.mt[1].issue, SIDE)
        step("project0", project, 0)
        step("M1cor", live.mt[1].issue, CORNER)
        step("downb0", down, 0, SECOND)
        step("comb0", combine, 0)
        step("project1", project, 1)
        step("comb1", combine, 1)
        step("comb3L", combine, 3, last=True)
        finish()

    @pl.when(inner == 0)
    def _():
        fresh()
        step("X0fwd", live.xt[0].issue, FORWARD)
        step("X0side", live.xt[0].issue, SIDE)
        step("ax1", x_arrived, 1)
        step("X1own", live.xt[1].issue, OWN)
        step("sx3", send_x, 3)
        step("X0cor", live.xt[0].issue, CORNER)
        step("hid0", hidden, 0)
        step("X1fwd", live.xt[1].issue, FORWARD)
        step("ax2", x_arrived, 2)
        step("X2own", live.xt[2].issue, OWN)
        step("X1side", live.xt[1].issue, SIDE)
        step("X1cor", live.xt[1].issue, CORNER)
        step("X2fwd", live.xt[2].issue, FORWARD)
        step("ax3", x_arrived, 3)
        step("X3own", live.xt[3].issue, OWN)
        step("sendkv", send_keys)
        step("hid1", hidden, 1)
        step("X2side", live.xt[2].issue, SIDE)
        step("queries", turn_queries)
        step("X2cor", live.xt[2].issue, CORNER)
        step("X3fwd", live.xt[3].issue, FORWARD)
        step("hid2", hidden, 2)
        on_core(0, "H2own", live.ht[2].issue, OWN)
        on_core(0, "H1own", live.ht[1].issue, OWN)
        step("X3side", live.xt[3].issue, SIDE)
        step("hida3", hidden, 3, FIRST, False)
        step("keyson", keys_on)
        step("X3cor", live.xt[3].issue, CORNER)
        on_core(1, "H2own", live.ht[2].issue, OWN)
        on_core(1, "H1own", live.ht[1].issue, OWN)
        step("H2fwd", live.ht[2].issue, FORWARD)
        step("hidb3", hidden, 3, SECOND)
        step("H3own", live.ht[3].issue, OWN)
        step("H2side", live.ht[2].issue, SIDE)
        step("wkv", keys_ready)
        step("att00", attention, 0, 0)
        step("H2cor", live.ht[2].issue, CORNER)
        step("H3fwd", live.ht[3].issue, FORWARD)
        step("H1fwd", live.ht[1].issue, FORWARD)
        step("down2", down, 2)
        step("H1side", live.ht[1].issue, SIDE)
        step("att01", attention, 0, 1)
        step("M0own", live.mt[0].issue, OWN)
        step("H3side", live.ht[3].issue, SIDE)
        step("att10", attention, 1, 0)
        step("H0own", live.ht[0].issue, OWN)
        step("downa3", down, 3, FIRST, False)
        step("H3cor", live.ht[3].issue, CORNER)
        step("downb3", down, 3, SECOND)
        step("H1cor", live.ht[1].issue, CORNER)
        step("att11", attention, 1, 1)
        step("M1own", live.mt[1].issue, OWN)
        step("M0fwd", live.mt[0].issue, FORWARD)
        step("down1", down, 1)
        step("M0side", live.mt[0].issue, SIDE)
        step("H0fwd", live.ht[0].issue, FORWARD)
        step("comb2F", combine, 2, first=True)
        step("M1fwd", live.mt[1].issue, FORWARD)
        step("M0cor", live.mt[0].issue, CORNER)
        step("H0side", live.ht[0].issue, SIDE)
        step("downa0", down, 0, FIRST, False)
        step("H0cor", live.ht[0].issue, CORNER)
        step("M1side", live.mt[1].issue, SIDE)
        step("project0", project, 0)
        step("M1cor", live.mt[1].issue, CORNER)
        step("downb0", down, 0, SECOND)
        step("comb0", combine, 0)
        step("project1", project, 1)
        step("comb1", combine, 1)
        step("comb3L", combine, 3, last=True)
        finish()


def hand_on(a_ref, b_ref, a_out, b_out, sems):
    copies = [
        pltpu.make_async_copy(a_ref, a_out, sems.at[0]),
        pltpu.make_async_copy(b_ref, b_out, sems.at[1]),
    ]
    for copy in copies:
        copy.start()
    for copy in copies:
        copy.wait()


def hand_out(outs):
    return pl.pallas_call(
        hand_on,
        out_shape=tuple(jax.ShapeDtypeStruct(o.shape, o.dtype) for o in outs),
        in_specs=[pl.BlockSpec(memory_space=pltpu.VMEM)] * 2,
        out_specs=[pl.BlockSpec(memory_space=pl.ANY)] * 2,
        scratch_shapes=[pltpu.SemaphoreType.DMA((2,))],
    )(*(pltpu.with_memory_space_constraint(o, pltpu.VMEM) for o in outs))


def shards(
    n_ep, n_tp,
    queries, key_rows, values, query_gain, key_gain, mix_gain, out_weight, expert_input,
    expert_gain, route_ids, route_weights, expert_gate, expert_up, expert_down,
):
    length, width = expert_input.shape
    qw, kw = queries.shape[1], key_rows.shape[1]
    ffw = expert_gate.shape[2]
    out_w = out_weight.shape[1]
    copies = length * route_ids.shape[1]
    capacity = (4 * copies + 3 * n_ep - 1) // (3 * n_ep)
    cap = (capacity + 15) // 16 * 16
    groups = 4
    rows = cap * (n_ep // groups)
    plan = gather_plan(n_tp)

    table_w = min(128, qw)
    operands = (
        queries, key_rows, values,
        query_gain.reshape(1, HEAD), key_gain.reshape(1, HEAD),
        mix_gain.reshape(n_tp, 1, qw),
        out_weight.reshape(n_tp, qw, out_w),
        expert_input,
        expert_gain.reshape(n_tp, 1, width),
        route_ids.T, route_weights.T,
        expert_gate.reshape(n_tp, width, ffw),
        expert_up.reshape(n_tp, width, ffw),
        expert_down.reshape(n_tp, ffw, out_w),
    )
    vmem = pl.BlockSpec(memory_space=pltpu.VMEM)
    hbm = pl.BlockSpec(memory_space=pl.ANY)
    specs = [hbm if i in (6, 11, 12, 13) else vmem for i in range(len(operands))]
    dma = pltpu.SemaphoreType.DMA
    line = n_ep == 4 and n_tp == 8
    tables_at = [pltpu.VMEM((length, table_w), F32)] * 2
    blocks_at = [
        pltpu.VMEM((n_ep, cap, width), BF16),
        pltpu.VMEM((groups, n_tp, rows, width), BF16),
        pltpu.VMEM((groups, n_tp, rows, ffw), BF16),
        pltpu.VMEM((n_tp, length, qw), BF16),
    ]
    weights_at = [
        pltpu.VMEM((n_tp, width, 2 * ffw), BF16),
        pltpu.VMEM((n_tp, ffw, out_w), BF16),
        pltpu.VMEM((n_tp, qw, out_w), BF16),
    ]
    results_at = [
        pltpu.VMEM((length, qw), BF16),
        pltpu.VMEM((groups, rows, out_w), BF16),
        pltpu.VMEM((n_ep, cap, out_w), BF16),
    ]
    if line:
        body = functools.partial(line_kernel, n_ep, n_tp, cap)
        scratch = tables_at + blocks_at + [pltpu.VMEM((n_ep, length, 2 * kw), BF16)]
        scratch += results_at + [pltpu.VMEM((2, length, out_w), F32)] + weights_at
        scratch += [dma((4,)), dma((3,)), dma((3, n_ep - 1)), dma((3,)), dma((2 * n_ep + 2, 4))]
    else:
        body = functools.partial(kernel, n_ep, n_tp, cap, plan)
        scratch = tables_at + blocks_at + [pltpu.VMEM((n_ep, length, kw), BF16)] * 2
        scratch += results_at + weights_at
        scratch += [dma((4, n_tp)), dma((1,))] + [dma((n_ep,))] * 8
        scratch += [dma((groups, len(plan)))] * 4 + [dma((len(plan),))] * 2
    outs = pl.pallas_call(
        body,
        out_shape=(
            pltpu.VMEM((length, out_w), BF16),
            pltpu.VMEM((length, out_w), BF16),
        ),
        in_specs=specs,
        out_specs=(vmem, vmem),
        scratch_shapes=scratch,
        compiler_params=pltpu.CompilerParams(
            collective_id=0, has_side_effects=True, vmem_limit_bytes=60 * 1024 * 1024
        ),
    )(*operands)
    return hand_out(outs)


def solution(mesh):
    placed = (
        P("ep", "tp"), P("ep", "tp"), P("ep", "tp"), P(), P(), P(), P(None, "tp"),
        P("ep", "tp"), P(), P("ep", None), P("ep", None),
        P("ep", None, "tp"), P("ep", None, "tp"), P("ep", None, "tp"),
    )
    return jax.shard_map(
        functools.partial(shards, mesh.shape["ep"], mesh.shape["tp"]),
        mesh=mesh,
        in_specs=placed,
        out_specs=(P("ep", "tp"), P("ep", "tp")),
        check_vma=False,
    )
```

```python
import functools
import math
import types

import jax
import jax.numpy as jnp
import numpy as np
from jax import lax
from jax.experimental import pallas as pl
from jax.experimental.pallas import tpu as pltpu
from jax.sharding import PartitionSpec as P

Q_HEADS = 32
KV_HEADS = 16
HEAD = 64
GRID_W = 64
EPS = 1e-06
THETA = 10000.0
MESH = pl.DeviceIdType.MESH
F32 = jnp.float32
BF16 = jnp.bfloat16


def gather_plan(n_tp):
    if n_tp == 8:
        return (
            (2, 0, None, None),
            (4, 0, None, None),
            (1, 0, None, None),
            (4, 2, 0, 0),
            (2, 4, 1, 1),
            (1, 2, None, 0),
            (1, 4, None, 1),
            (1, 6, 0, 3),
            (1, 6, 1, 4),
        )
    return tuple((m, 0, None, None) for m in range(1, n_tp))


def plan_stages(plan):
    depth = []
    for entry in plan:
        depth.append(0 if entry[3] is None else depth[entry[3]] + 1)
    return [[i for i, d in enumerate(depth) if d == k] for k in range(3)]


class Gather:
    def __init__(self, name, plan, buf, send, recv, tp):
        self.name = name
        self.plan, self.buf, self.send, self.recv, self.tp = plan, buf, send, recv, tp
        self.stages = plan_stages(plan)
        self.waited = set()
        self.sent = []

    def part(self, block, half):
        if half is None:
            return self.buf.at[block]
        width = self.buf.shape[-1] // 2
        return self.buf.at[block, :, pl.ds(half * width, width)]

    def copy(self, i):
        target, block, half, _ = self.plan[i]
        return pltpu.make_async_remote_copy(
            src_ref=self.part(block, half),
            dst_ref=self.part(block ^ target, half),
            send_sem=self.send.at[i],
            recv_sem=self.recv.at[i],
            device_id={"tp": self.tp ^ target},
            device_id_type=MESH,
        )

    def wait_entry(self, i):
        if i not in self.waited:
            self.waited.add(i)
            with jax.named_scope(f"w{self.name}_{i}"):
                self.copy(i).wait_recv()

    def stage(self, k):
        for i in self.stages[k]:
            if self.plan[i][3] is not None:
                self.wait_entry(self.plan[i][3])
            copy = self.copy(i)
            copy.start()
            self.sent.append(copy)

    def ready(self, block):
        for i, entry in enumerate(self.plan):
            if entry[1] ^ entry[0] == block:
                self.wait_entry(i)

    def order(self):
        blocks = [0]
        for entry in self.plan:
            if entry[0] ^ entry[1] not in blocks:
                blocks.append(entry[0] ^ entry[1])
        return blocks

    def drain(self):
        for copy in self.sent:
            copy.wait_send()


def iota(shape, axis):
    return lax.broadcasted_iota(jnp.int32, shape, axis)


def exact_dot(a, b):
    return jnp.dot(a, b, precision=lax.Precision.HIGHEST, preferred_element_type=F32)


def norm_turn(source, gain, cosine, sine):
    width = source.shape[1]
    rows = source.astype(F32)
    i0, i1 = iota((width, width), 0), iota((width, width), 1)
    same_head = jnp.where(i0 // HEAD == i1 // HEAD, 1.0 / HEAD, 0.0).astype(F32)
    mean = exact_dot(rows * rows, same_head)
    rows = rows * lax.rsqrt(mean + EPS) * gain
    partner = jnp.where(i1 % 2 == 0, i1 + 1, i1 - 1)
    sign = jnp.where(i1 % 2 == 0, -1.0, 1.0)
    swap = jnp.where(i0 == partner, sign, 0.0).astype(F32)
    return rows * cosine + exact_dot(rows, swap) * sine


def tables(cos_ref, sin_ref, offset):
    length, width = cos_ref.shape
    half_width = HEAD // 2
    inverse = THETA ** (-np.arange(0, half_width, 2, dtype=np.float32) / half_width)
    pair = iota((1, width), 1) % HEAD // 2
    row_inv = jnp.zeros((1, width), F32)
    for m, value in enumerate(inverse.astype(np.float32)):
        row_inv = jnp.where(pair % len(inverse) == m, float(value), row_inv)
    position = offset + iota((length, width), 0)
    grid = jnp.where(
        iota((length, width), 1) % HEAD < half_width, position // GRID_W, position % GRID_W
    ).astype(F32)
    angle = grid * row_inv
    cos_ref[...] = jnp.cos(angle)
    sin_ref[...] = jnp.sin(angle)


def kernel(
    n_ep, n_tp, cap, plan,
    q_ref, k_ref, v_ref, qg_ref, kg_ref, mg_ref, wo_hbm, x_ref, xg_ref,
    idst_ref, rwt_ref, wg_hbm, wu_hbm, wd_hbm,
    att_ref, mix_ref,
    cos_ref, sin_ref, xo, xb, hb, mb, kb, vb, qb, ob, rb, wgu, wd, wo,
    w_sem, v_sem,
    xz_send, xz_recv, kz_send, kz_recv, vz_send, vz_recv, rz_send, rz_recv,
    xt_send, xt_recv, ht_send, ht_recv, mt_send, mt_recv,
):
    ep, tp = lax.axis_index("ep"), lax.axis_index("tp")
    groups = xb.shape[0]
    per = n_ep // groups
    length = x_ref.shape[0]
    ffw = hb.shape[-1]

    barrier = pltpu.get_barrier_semaphore()
    for d in range(1, n_ep):
        pl.semaphore_signal(barrier, inc=1, device_id={"ep": ep ^ d}, device_id_type=MESH)
    for m in range(1, n_tp):
        pl.semaphore_signal(barrier, inc=1, device_id={"tp": tp ^ m}, device_id_type=MESH)

    lanes = (n_ep + 15) // 16 * 16
    hit_t = [(idst_ref[k : k + 1, :] == iota((lanes, length), 0)) for k in range(2)]
    both_t = sum(jnp.where(h, 1.0, 0.0) for h in hit_t).astype(BF16)
    i0, i1 = iota((length, length), 0), iota((length, length), 1)
    before_t = jnp.where(i0 < i1, 1.0, 0.0).astype(BF16)
    count_t = jnp.dot(both_t, before_t, preferred_element_type=F32)
    slot_t = [
        jnp.sum(jnp.where(hit_t[k], count_t, 0.0), axis=0, keepdims=True).astype(jnp.int32)
        + idst_ref[k : k + 1, :] * cap
        for k in range(2)
    ]

    def picked_rows(d):
        index = (ep ^ d) * cap + iota((cap, length), 0)
        choose = jnp.where((slot_t[0] == index) | (slot_t[1] == index), 1.0, 0.0).astype(BF16)
        return jnp.dot(choose, x_ref[...], preferred_element_type=F32).astype(BF16)

    sends = []

    def ep_copy(source, target, d, send, recv):
        return pltpu.make_async_remote_copy(
            src_ref=source, dst_ref=target, send_sem=send.at[d], recv_sem=recv.at[d],
            device_id={"ep": ep ^ d}, device_id_type=MESH,
        )

    def x_copy(d):
        return ep_copy(
            xo.at[d], xb.at[d // per, 0, pl.ds((d % per) * cap, cap)], d, xz_send, xz_recv
        )

    xt = [Gather(f"x{c}", plan, xb.at[c], xt_send.at[c], xt_recv.at[c], tp) for c in range(groups)]
    ht = [Gather(f"h{c}", plan, hb.at[c], ht_send.at[c], ht_recv.at[c], tp) for c in range(groups)]
    mt = Gather("m", plan, mb, mt_send, mt_recv, tp)

    xb[0, 0, pl.ds(0, cap), :] = picked_rows(0)
    pl.semaphore_wait(barrier, n_ep + n_tp - 2)
    if per == 1:
        xt[0].stage(0)

    def send_rows(c):
        for d in range(c * per, (c + 1) * per):
            if d:
                copy = x_copy(d)
                copy.start()
                sends.append(copy)

    for d in range(1, n_ep):
        xo[d] = picked_rows(d)
        if d == max(per - 1, 1):
            for c in range(0 if per > 1 else 1, 1 if per > 1 else 2):
                send_rows(c)

    def x_first(c):
        for d in range(c * per, (c + 1) * per):
            if d:
                x_copy(d).wait_recv()
        xt[c].stage(0)

    local = []
    for m in range(n_tp):
        p = tp ^ m
        pieces = (
            (wg_hbm.at[p], wgu.at[m, :, pl.ds(0, ffw)]),
            (wu_hbm.at[p], wgu.at[m, :, pl.ds(ffw, ffw)]),
            (wd_hbm.at[p], wd.at[m]),
            (wo_hbm.at[p], wo.at[m]),
        )
        for k, (source, target) in enumerate(pieces):
            copy = pltpu.make_async_copy(source, target, w_sem.at[k, m])
            copy.start()
            local.append(((k, m), copy))
    local = dict(local)
    own_v = pltpu.make_async_copy(v_ref, vb.at[0], v_sem.at[0])
    own_v.start()

    if per > 1:
        x_first(0)

    tables(cos_ref, sin_ref, ep * length)
    kb[0] = norm_turn(
        k_ref[...],
        jnp.concatenate([kg_ref[...]] * (k_ref.shape[1] // HEAD), axis=1),
        cos_ref[:, : k_ref.shape[1]],
        sin_ref[:, : k_ref.shape[1]],
    ).astype(BF16)
    own_v.wait()

    def send_keys():
        for d in range(1, n_ep):
            for source, target, send, recv in (
                (kb.at[0], kb.at[d], kz_send, kz_recv),
                (vb.at[0], vb.at[d], vz_send, vz_recv),
            ):
                copy = ep_copy(source, target, d, send, recv)
                copy.start()
                sends.append(copy)

    def turn_queries():
        qw = cos_ref.shape[1]
        gain = jnp.concatenate([qg_ref[...]] * (qw // HEAD), axis=1)
        for i in range(q_ref.shape[1] // qw):
            part = pl.ds(i * qw, qw)
            turned = norm_turn(q_ref[:, part], gain, cos_ref[...], sin_ref[...])
            qb[:, part] = (turned.astype(BF16).astype(F32) * (1.0 / math.sqrt(HEAD))).astype(BF16)

    fetched = set()

    def weights(k, m):
        if (k, m) not in fetched:
            fetched.add((k, m))
            local[k, m].wait()

    def hidden(c):
        rows = xb.shape[2]
        total = jnp.zeros((rows, 2 * ffw), F32)
        squares = jnp.zeros((rows, 1), F32)
        for m in xt[c].order():
            xt[c].ready(m)
            weights(0, m)
            weights(1, m)
            block = xb[c, m].astype(F32)
            squares += jnp.sum(block * block, axis=1, keepdims=True)
            scaled = (block * xg_ref[tp ^ m]).astype(BF16)
            total += jnp.dot(scaled, wgu[m], preferred_element_type=F32)
        stat = lax.rsqrt(squares / xg_ref.shape[0] / xg_ref.shape[2] + EPS)
        gate = total[:, :ffw] * stat
        up = total[:, ffw:] * stat
        hb[c, 0] = (gate / (1.0 + jnp.exp(-gate)) * up).astype(BF16)

    def r_copy(d):
        return ep_copy(
            ob.at[d // per, pl.ds((d % per) * cap, cap)], rb.at[d], d, rz_send, rz_recv
        )

    def down(c):
        total = jnp.zeros((ob.shape[1], ob.shape[2]), F32)
        for m in ht[c].order():
            ht[c].ready(m)
            weights(2, m)
            total += jnp.dot(hb[c, m], wd[m], preferred_element_type=F32)
        ob[c] = total.astype(BF16)
        for d in range(c * per, (c + 1) * per):
            if d:
                copy = r_copy(d)
                copy.start()
                sends.append(copy)

    def keys_ready():
        for d in range(1, n_ep):
            ep_copy(kb.at[0], kb.at[d], d, kz_send, kz_recv).wait_recv()
            ep_copy(vb.at[0], vb.at[d], d, vz_send, vz_recv).wait_recv()

    def attention(part):
        keys = n_ep * length
        block = length // 2
        rows = pl.ds(part * block, block)
        outs = []
        for h in range(q_ref.shape[1] // HEAD):
            g = h * KV_HEADS // Q_HEADS
            lane = pl.ds(g * HEAD, HEAD)
            query = qb[rows, pl.ds(h * HEAD, HEAD)]
            key = kb[:, :, lane].reshape(keys, HEAD)
            value = vb[:, :, lane].reshape(keys, HEAD)
            scores = lax.dot_general(
                query, key, (((1,), (1,)), ((), ())), preferred_element_type=F32
            )
            raw = jnp.exp(scores - jnp.max(scores, axis=1, keepdims=True))
            total = jnp.sum(raw, axis=1, keepdims=True)
            out = jnp.dot(raw.astype(BF16), value, preferred_element_type=F32)
            outs.append(out / total)
        mb[0, rows, :] = jnp.concatenate(outs, axis=1).astype(BF16)

    def project():
        total = jnp.zeros(att_ref.shape, F32)
        squares = jnp.zeros((length, 1), F32)
        for m in mt.order():
            mt.ready(m)
            weights(3, m)
            block = mb[m].astype(F32)
            squares += jnp.sum(block * block, axis=1, keepdims=True)
            scaled = (block * mg_ref[tp ^ m]).astype(BF16)
            total += jnp.dot(scaled, wo[m], preferred_element_type=F32)
        scale = lax.rsqrt(squares / mg_ref.shape[0] / mg_ref.shape[2] + EPS)
        att_ref[...] = (total * scale).astype(BF16)

    def combine():
        stack = jnp.concatenate(
            [slot_t[0].astype(F32), slot_t[1].astype(F32), rwt_ref[...]] * 2, axis=0
        )
        columns = lax.dot_general(
            jnp.where(i0 == i1, 1.0, 0.0).astype(F32), stack, (((1,), (1,)), ((), ())),
            precision=lax.Precision.HIGHEST, preferred_element_type=F32,
        )
        slot = [(columns[:, k : k + 1] + 0.5).astype(jnp.int32) for k in range(2)]
        total = [jnp.zeros(mix_ref.shape, F32) for k in range(2)]
        for d in range(n_ep):
            if d:
                r_copy(d).wait_recv()
                back = rb[d]
            else:
                back = ob[0, pl.ds(0, cap), :]
            index = (ep ^ d) * cap + iota((length, cap), 1)
            for k in range(2):
                choose = jnp.where(slot[k] == index, 1.0, 0.0).astype(BF16)
                total[k] += jnp.dot(choose, back, preferred_element_type=F32)
        mix_ref[...] = (total[0] * columns[:, 2:3] + total[1] * columns[:, 3:4]).astype(BF16)


    if per > 1:
        send_rows(1)
    send_rows(2)
    xt[0].stage(1)
    x_first(1)
    send_rows(3)
    xt[0].stage(2)
    turn_queries()
    hidden(0)
    ht[0].stage(0)
    xt[1].stage(1)
    ht[0].stage(1)
    xt[1].stage(2)
    x_first(2)
    send_keys()
    hidden(1)
    ht[1].stage(0)
    ht[0].stage(2)
    xt[2].stage(1)
    x_first(3)
    down(0)
    ht[1].stage(1)
    xt[2].stage(2)
    hidden(2)
    ht[2].stage(0)
    xt[3].stage(1)
    ht[1].stage(2)
    down(1)
    ht[2].stage(1)
    keys_ready()
    attention(0)
    xt[3].stage(2)
    ht[2].stage(2)
    hidden(3)
    ht[3].stage(0)
    down(2)
    attention(1)
    ht[3].stage(1)
    mt.stage(0)
    ht[3].stage(2)
    down(3)
    mt.stage(1)
    mt.stage(2)
    project()
    combine()

    for copy in sends:
        copy.wait_send()
    for gather in xt + ht + [mt]:
        gather.drain()


RELAY_PLAN = (
    (2, 0, 0),
    (4, 0, 1),
    (2, 0, 1),
    (4, 0, 0),
    (4, 2, 0),
    (2, 4, 1),
    (1, 0, None),
    (1, 2, None),
    (1, 4, None),
    (1, 6, None),
)
RELAY_WAIT = (0, 0, 1, 1, 2, 2, 3, 3, 3, 3)
OWN = (0, 1, 2, 3, 6)
LEAD = (0, 1)
REST = (2, 3, 6)
FORWARD = (4, 5)
SIDE = (7, 8)
CORNER = (9,)
NEEDS = {FORWARD: 0, SIDE: 1, CORNER: 2}
NEAR = (0, 2, 4, 6)
FAR = (1, 3, 5, 7)
FIRST = NEAR[:3]
SECOND = NEAR[3:] + FAR


class Relay:
    def __init__(self, name, buf, send, recv, tp):
        self.name = name
        self.buf, self.send, self.recv, self.tp = buf, send, recv, tp
        self.waited = set()

    def part(self, block, half):
        if half is None:
            return self.buf.at[block]
        width = self.buf.shape[-1] // 2
        return self.buf.at[block, :, pl.ds(half * width, width)]

    def copy(self, i):
        target, block, half = RELAY_PLAN[i]
        return pltpu.make_async_remote_copy(
            src_ref=self.part(block, half),
            dst_ref=self.part(block ^ target, half),
            send_sem=self.send,
            recv_sem=self.recv.at[RELAY_WAIT[i]],
            device_id={"tp": self.tp ^ target},
            device_id_type=MESH,
        )

    def whole(self, blocks, i):
        part = self.buf.at[pl.ds(0, blocks)]
        return pltpu.make_async_remote_copy(
            src_ref=part, dst_ref=part, send_sem=self.send, recv_sem=self.recv.at[i],
            device_id={"tp": self.tp ^ 1}, device_id_type=MESH,
        )

    def wait(self, i):
        if i not in self.waited:
            self.waited.add(i)
            with jax.named_scope(f"w{self.name}_{i}"):
                self.whole(len(FAR) if i == 3 else 1, i).wait_recv()

    def issue(self, entries):
        if entries in NEEDS:
            self.wait(NEEDS[entries])
        for i in entries:
            self.copy(i).start()

    def ready(self, block):
        if block in FAR:
            self.wait(3)
        elif block:
            for i in (0, 1, 2) if block in SECOND else (0, 1):
                self.wait(i)


def line_kernel(
    n_ep, n_tp, cap,
    q_ref, k_ref, v_ref, qg_ref, kg_ref, mg_ref, wo_hbm, x_ref, xg_ref,
    idst_ref, rwt_ref, wg_hbm, wu_hbm, wd_hbm,
    att_ref, mix_ref,
    cos_ref, sin_ref, xo, xb, hb, mb, kv, qb, ob, rb, ct, wgu, wd, wo,
    w_sem, z_send, z_recv, t_send, t_recv,
):
    ep, tp = lax.axis_index("ep"), lax.axis_index("tp")
    length = x_ref.shape[0]
    ffw = hb.shape[-1]
    kw = k_ref.shape[1]
    half = length // 2
    inner = (ep + 1) // 2 % 2

    barrier = pltpu.get_barrier_semaphore()
    for d in range(1, n_ep):
        pl.semaphore_signal(barrier, inc=1, device_id={"ep": ep ^ d}, device_id_type=MESH)
    for m in range(1, n_tp):
        pl.semaphore_signal(barrier, inc=1, device_id={"tp": tp ^ m}, device_id_type=MESH)

    lanes = (n_ep + 15) // 16 * 16
    hit_t = [(idst_ref[k : k + 1, :] == iota((lanes, length), 0)) for k in range(2)]
    both_t = sum(jnp.where(h, 1.0, 0.0) for h in hit_t).astype(BF16)
    i0, i1 = iota((length, length), 0), iota((length, length), 1)
    before_t = jnp.where(i0 < i1, 1.0, 0.0).astype(BF16)
    count_t = jnp.dot(both_t, before_t, preferred_element_type=F32)
    slot_t = [
        jnp.sum(jnp.where(hit_t[k], count_t, 0.0), axis=0, keepdims=True).astype(jnp.int32)
        + idst_ref[k : k + 1, :] * cap
        for k in range(2)
    ]

    def picked_rows(d):
        index = (ep ^ d) * cap + iota((cap, length), 0)
        choose = jnp.where((slot_t[0] == index) | (slot_t[1] == index), 1.0, 0.0).astype(BF16)
        return jnp.dot(choose, x_ref[...], preferred_element_type=F32).astype(BF16)

    def ep_copy(source, target, d, send, recv):
        return pltpu.make_async_remote_copy(
            src_ref=source, dst_ref=target, send_sem=send, recv_sem=recv,
            device_id={"ep": ep ^ d}, device_id_type=MESH,
        )

    def x_copy(d):
        return ep_copy(xo.at[d], xb.at[d, 0], d, z_send.at[0], z_recv.at[0, d - 1])

    def r_copy(d):
        return ep_copy(ob.at[d], rb.at[d], d, z_send.at[1], z_recv.at[1, d - 1])

    def kv_copy(i):
        d, block = ((1, 0), (2, 0), (1, 2))[i]
        return ep_copy(kv.at[block], kv.at[block ^ d], d, z_send.at[2], z_recv.at[2, i])

    live = types.SimpleNamespace()

    def fresh():
        live.fetched = set()
        live.partial = {}
        live.xt = [
            Relay(f"x{d}", xb.at[d], t_send.at[0], t_recv.at[d], tp) for d in range(n_ep)
        ]
        live.ht = [
            Relay(f"h{d}", hb.at[d], t_send.at[1], t_recv.at[n_ep + d], tp) for d in range(n_ep)
        ]
        live.mt = [
            Relay(
                f"m{k}", mb.at[:, pl.ds(k * half, half)],
                t_send.at[2], t_recv.at[2 * n_ep + k], tp,
            )
            for k in range(2)
        ]

    pieces = (
        (wg_hbm, wgu.at[:, :, pl.ds(0, ffw)]),
        (wu_hbm, wgu.at[:, :, pl.ds(ffw, ffw)]),
        (wd_hbm, wd),
        (wo_hbm, wo),
    )
    local = [
        pltpu.make_async_copy(source, target, w_sem.at[k])
        for k, (source, target) in enumerate(pieces)
    ]
    def weights(k):
        if k not in live.fetched:
            live.fetched.add(k)
            with jax.named_scope(f"ww_{k}"):
                local[k].wait()

    def own_keys():
        tables(cos_ref, sin_ref, ep * length)
        kv[0, :, pl.ds(kw, kw)] = v_ref[...]
        kv[0, :, pl.ds(0, kw)] = norm_turn(
            k_ref[...],
            jnp.concatenate([kg_ref[...]] * (kw // HEAD), axis=1),
            cos_ref[:, :kw],
            sin_ref[:, :kw],
        ).astype(BF16)

    def send_keys():
        kv_copy(0).start()
        kv_copy(1).start()

    def keys_on():
        with jax.named_scope("wkv_1"):
            kv_copy(1).wait_recv()
        kv_copy(2).start()

    def keys_ready():
        with jax.named_scope("wkv_0"):
            kv_copy(0).wait_recv()
        with jax.named_scope("wkv_2"):
            kv_copy(2).wait_recv()

    def turn_queries():
        qw = cos_ref.shape[1]
        gain = jnp.concatenate([qg_ref[...]] * (qw // HEAD), axis=1)
        for i in range(q_ref.shape[1] // qw):
            part = pl.ds(i * qw, qw)
            turned = norm_turn(q_ref[:, part], gain, cos_ref[...], sin_ref[...])
            qb[:, part] = (turned.astype(BF16).astype(F32) * (1.0 / math.sqrt(HEAD))).astype(BF16)

    def x_arrived(d):
        with jax.named_scope(f"wxz_{d}"):
            x_copy(d).wait_recv()

    def hidden(d, blocks=NEAR + FAR, last=True):
        total, squares = live.partial.pop(("x", d), (None, None))
        for m in blocks:
            live.xt[d].ready(m)
            weights(0)
            weights(1)
            block = xb[d, m].astype(F32)
            square = jnp.sum(block * block, axis=1, keepdims=True)
            scaled = (block * xg_ref[tp ^ m]).astype(BF16)
            product = jnp.dot(scaled, wgu[tp ^ m], preferred_element_type=F32)
            total = product if total is None else total + product
            squares = square if squares is None else squares + square
        if not last:
            live.partial["x", d] = total, squares
            return
        stat = lax.rsqrt(squares / xg_ref.shape[0] / xg_ref.shape[2] + EPS)
        gate = total[:, :ffw] * stat
        up = total[:, ffw:] * stat
        hb[d, 0] = (gate / (1.0 + jnp.exp(-gate)) * up).astype(BF16)

    def down(d, blocks=NEAR + FAR, last=True):
        total = live.partial.pop(("h", d), None)
        for m in blocks:
            live.ht[d].ready(m)
            weights(2)
            product = jnp.dot(hb[d, m], wd[tp ^ m], preferred_element_type=F32)
            total = product if total is None else total + product
        if not last:
            live.partial["h", d] = total
            return
        ob[d] = total.astype(BF16)
        if d:
            r_copy(d).start()

    def attention(part, pair):
        keys = n_ep * length
        rows = pl.ds(part * half, half)
        outs = []
        for h in range(2 * pair, 2 * pair + 2):
            g = h * KV_HEADS // Q_HEADS
            query = qb[rows, pl.ds(h * HEAD, HEAD)]
            key = kv[:, :, pl.ds(g * HEAD, HEAD)].reshape(keys, HEAD)
            value = kv[:, :, pl.ds(kw + g * HEAD, HEAD)].reshape(keys, HEAD)
            scores = lax.dot_general(
                query, key, (((1,), (1,)), ((), ())), preferred_element_type=F32
            )
            raw = jnp.exp(scores - jnp.max(scores, axis=1, keepdims=True))
            total = jnp.sum(raw, axis=1, keepdims=True)
            out = jnp.dot(raw.astype(BF16), value, preferred_element_type=F32)
            outs.append(out / total)
        lane = pl.ds(2 * pair * HEAD, 2 * HEAD)
        mb[0, rows, lane] = jnp.concatenate(outs, axis=1).astype(BF16)

    def project(part):
        rows = pl.ds(part * half, half)
        total = jnp.zeros((half, att_ref.shape[1]), F32)
        squares = jnp.zeros((half, 1), F32)
        for m in NEAR + FAR:
            live.mt[part].ready(m)
            weights(3)
            block = mb[m, rows, :].astype(F32)
            squares += jnp.sum(block * block, axis=1, keepdims=True)
            scaled = (block * mg_ref[tp ^ m]).astype(BF16)
            total += jnp.dot(scaled, wo[tp ^ m], preferred_element_type=F32)
        scale = lax.rsqrt(squares / mg_ref.shape[0] / mg_ref.shape[2] + EPS)
        att_ref[rows, :] = (total * scale).astype(BF16)

    places = {}

    def columns():
        stack = jnp.concatenate(
            [slot_t[0].astype(F32), slot_t[1].astype(F32), rwt_ref[...]] * 2, axis=0
        )
        column = lax.dot_general(
            jnp.where(i0 == i1, 1.0, 0.0).astype(F32), stack, (((1,), (1,)), ((), ())),
            precision=lax.Precision.HIGHEST, preferred_element_type=F32,
        )
        places["slot"] = [(column[:, k : k + 1] + 0.5).astype(jnp.int32) for k in range(2)]
        places["weight"] = [column[:, 2 + k : 3 + k] for k in range(2)]

    def combine(d, first=False, last=False):
        index = (ep ^ d) * cap + iota((length, cap), 1)
        choose = [
            jnp.where(places["slot"][k] == index, 1.0, 0.0).astype(BF16) for k in range(2)
        ]
        if d:
            with jax.named_scope(f"wr_{d}"):
                r_copy(d).wait_recv()
        back = rb[d] if d else ob[0]
        total = []
        for k in range(2):
            found = jnp.dot(choose[k], back, preferred_element_type=F32)
            total.append(found if first else ct[k] + found)
        if last:
            weight = places["weight"]
            mix_ref[...] = (total[0] * weight[0] + total[1] * weight[1]).astype(BF16)
        else:
            for k in range(2):
                ct[k] = total[k]

    def step(name, f, *args, **kwargs):
        with jax.named_scope("S_" + name):
            f(*args, **kwargs)

    def on_core(core, name, f, *args):
        @pl.when(tp % 2 == core)
        def _():
            step(name, f, *args)

    def pick_x(d):
        xo[d] = picked_rows(d)

    def send_x(d):
        if d == 3:
            pick_x(d)
        x_copy(d).start()

    def finish():
        with jax.named_scope("S_drain"):
            for i, buf in enumerate((xo, rb, kv)):
                part = buf.at[pl.ds(0, n_ep - 1)]
                ep_copy(part, part, 1, z_send.at[i], z_recv.at[i, 0]).wait_send()
            sent = pl.ds(0, n_tp - 1)
            for i, part in enumerate((xb.at[:, sent], hb.at[:, sent], mb.at[sent])):
                pltpu.make_async_remote_copy(
                    src_ref=part, dst_ref=part, send_sem=t_send.at[i], recv_sem=t_recv.at[0, 0],
                    device_id={"tp": tp ^ 1}, device_id_type=MESH,
                ).wait_send()

    for copy in local:
        copy.start()
    xb[0, 0] = picked_rows(0)
    pick_x(2)
    pick_x(1)
    with jax.named_scope("S_barrier"):
        pl.semaphore_wait(barrier, n_ep + n_tp - 2)
    fresh()
    step("sx2", send_x, 2)
    step("sx1", send_x, 1)
    step("X0lead", live.xt[0].issue, LEAD)
    step("keys", own_keys)
    step("X0rest", live.xt[0].issue, REST)
    step("columns", columns)

    @pl.when(inner == 1)
    def _():
        fresh()
        step("X0fwd", live.xt[0].issue, FORWARD)
        step("X0side", live.xt[0].issue, SIDE)
        step("ax2", x_arrived, 2)
        step("X2own", live.xt[2].issue, OWN)
        step("sx3", send_x, 3)
        step("X0cor", live.xt[0].issue, CORNER)
        step("hid0", hidden, 0)
        step("X2fwd", live.xt[2].issue, FORWARD)
        step("ax1", x_arrived, 1)
        step("X1own", live.xt[1].issue, OWN)
        step("X2side", live.xt[2].issue, SIDE)
        step("X2cor", live.xt[2].issue, CORNER)
        step("X1fwd", live.xt[1].issue, FORWARD)
        step("hid2", hidden, 2)
        step("H2own", live.ht[2].issue, OWN)
        step("ax3", x_arrived, 3)
        step("sendkv", send_keys)
        step("X3lead", live.xt[3].issue, LEAD)
        step("X1side", live.xt[1].issue, SIDE)
        step("X1cor", live.xt[1].issue, CORNER)
        step("H2fwd", live.ht[2].issue, FORWARD)
        step("X3rest", live.xt[3].issue, REST)
        step("H2side", live.ht[2].issue, SIDE)
        step("queries", turn_queries)
        step("keyson", keys_on)
        step("hid1", hidden, 1)
        step("X3fwd", live.xt[3].issue, FORWARD)
        step("H1own", live.ht[1].issue, OWN)
        step("H2cor", live.ht[2].issue, CORNER)
        step("down2", down, 2)
        step("X3side", live.xt[3].issue, SIDE)
        step("wkv", keys_ready)
        step("att00", attention, 0, 0)
        step("X3cor", live.xt[3].issue, CORNER)
        step("H1fwd", live.ht[1].issue, FORWARD)
        step("hid3", hidden, 3)
        step("H3own", live.ht[3].issue, OWN)
        step("H1side", live.ht[1].issue, SIDE)
        step("att01", attention, 0, 1)
        on_core(0, "M0own", live.mt[0].issue, OWN)
        step("H1cor", live.ht[1].issue, CORNER)
        step("att10", attention, 1, 0)
        on_core(1, "M0own", live.mt[0].issue, OWN)
        step("H3fwd", live.ht[3].issue, FORWARD)
        step("down1", down, 1)
        step("att11", attention, 1, 1)
        step("H0own", live.ht[0].issue, OWN)
        step("M0fwd", live.mt[0].issue, FORWARD)
        step("M1own", live.mt[1].issue, OWN)
        step("H3side", live.ht[3].issue, SIDE)
        step("downa3", down, 3, FIRST, False)
        step("H3cor", live.ht[3].issue, CORNER)
        step("M0side", live.mt[0].issue, SIDE)
        step("downb3", down, 3, SECOND)
        step("comb2F", combine, 2, first=True)
        step("H0fwd", live.ht[0].issue, FORWARD)
        step("M0cor", live.mt[0].issue, CORNER)
        step("M1fwd", live.mt[1].issue, FORWARD)
        step("H0side", live.ht[0].issue, SIDE)
        step("downa0", down, 0, FIRST, False)
        step("H0cor", live.ht[0].issue, CORNER)
        step("M1side", live.mt[1].issue, SIDE)
        step("project0", project, 0)
        step("M1cor", live.mt[1].issue, CORNER)
        step("downb0", down, 0, SECOND)
        step("comb0", combine, 0)
        step("project1", project, 1)
        step("comb1", combine, 1)
        step("comb3L", combine, 3, last=True)
        finish()

    @pl.when(inner == 0)
    def _():
        fresh()
        step("X0fwd", live.xt[0].issue, FORWARD)
        step("X0side", live.xt[0].issue, SIDE)
        step("ax1", x_arrived, 1)
        step("X1own", live.xt[1].issue, OWN)
        step("sx3", send_x, 3)
        step("X0cor", live.xt[0].issue, CORNER)
        step("hid0", hidden, 0)
        step("X1fwd", live.xt[1].issue, FORWARD)
        step("ax2", x_arrived, 2)
        step("X2own", live.xt[2].issue, OWN)
        step("X1side", live.xt[1].issue, SIDE)
        step("X1cor", live.xt[1].issue, CORNER)
        step("X2fwd", live.xt[2].issue, FORWARD)
        step("ax3", x_arrived, 3)
        step("X3own", live.xt[3].issue, OWN)
        step("sendkv", send_keys)
        step("hid1", hidden, 1)
        step("X2side", live.xt[2].issue, SIDE)
        step("queries", turn_queries)
        step("X2cor", live.xt[2].issue, CORNER)
        step("X3fwd", live.xt[3].issue, FORWARD)
        step("hid2", hidden, 2)
        on_core(0, "H2own", live.ht[2].issue, OWN)
        on_core(0, "H1own", live.ht[1].issue, OWN)
        step("X3side", live.xt[3].issue, SIDE)
        step("hida3", hidden, 3, FIRST, False)
        step("keyson", keys_on)
        step("X3cor", live.xt[3].issue, CORNER)
        on_core(1, "H2own", live.ht[2].issue, OWN)
        on_core(1, "H1own", live.ht[1].issue, OWN)
        step("H2fwd", live.ht[2].issue, FORWARD)
        step("hidb3", hidden, 3, SECOND)
        step("H3own", live.ht[3].issue, OWN)
        step("H2side", live.ht[2].issue, SIDE)
        step("wkv", keys_ready)
        step("att00", attention, 0, 0)
        step("H2cor", live.ht[2].issue, CORNER)
        step("H3fwd", live.ht[3].issue, FORWARD)
        step("H1fwd", live.ht[1].issue, FORWARD)
        step("down2", down, 2)
        step("H1side", live.ht[1].issue, SIDE)
        step("att01", attention, 0, 1)
        step("M0own", live.mt[0].issue, OWN)
        step("H3side", live.ht[3].issue, SIDE)
        step("att10", attention, 1, 0)
        step("H0own", live.ht[0].issue, OWN)
        step("downa3", down, 3, FIRST, False)
        step("H3cor", live.ht[3].issue, CORNER)
        step("downb3", down, 3, SECOND)
        step("H1cor", live.ht[1].issue, CORNER)
        step("att11", attention, 1, 1)
        step("M1own", live.mt[1].issue, OWN)
        step("M0fwd", live.mt[0].issue, FORWARD)
        step("down1", down, 1)
        step("M0side", live.mt[0].issue, SIDE)
        step("H0fwd", live.ht[0].issue, FORWARD)
        step("comb2F", combine, 2, first=True)
        step("M1fwd", live.mt[1].issue, FORWARD)
        step("M0cor", live.mt[0].issue, CORNER)
        step("H0side", live.ht[0].issue, SIDE)
        step("downa0", down, 0, FIRST, False)
        step("H0cor", live.ht[0].issue, CORNER)
        step("M1side", live.mt[1].issue, SIDE)
        step("project0", project, 0)
        step("M1cor", live.mt[1].issue, CORNER)
        step("downb0", down, 0, SECOND)
        step("comb0", combine, 0)
        step("project1", project, 1)
        step("comb1", combine, 1)
        step("comb3L", combine, 3, last=True)
        finish()


def hand_on(a_ref, b_ref, a_out, b_out, sems):
    copies = [
        pltpu.make_async_copy(a_ref, a_out, sems.at[0]),
        pltpu.make_async_copy(b_ref, b_out, sems.at[1]),
    ]
    for copy in copies:
        copy.start()
    for copy in copies:
        copy.wait()


def hand_out(outs):
    return pl.pallas_call(
        hand_on,
        out_shape=tuple(jax.ShapeDtypeStruct(o.shape, o.dtype) for o in outs),
        in_specs=[pl.BlockSpec(memory_space=pltpu.VMEM)] * 2,
        out_specs=[pl.BlockSpec(memory_space=pl.ANY)] * 2,
        scratch_shapes=[pltpu.SemaphoreType.DMA((2,))],
    )(*(pltpu.with_memory_space_constraint(o, pltpu.VMEM) for o in outs))


def shards(
    n_ep, n_tp,
    queries, key_rows, values, query_gain, key_gain, mix_gain, out_weight, expert_input,
    expert_gain, route_ids, route_weights, expert_gate, expert_up, expert_down,
):
    length, width = expert_input.shape
    qw, kw = queries.shape[1], key_rows.shape[1]
    ffw = expert_gate.shape[2]
    out_w = out_weight.shape[1]
    copies = length * route_ids.shape[1]
    capacity = (4 * copies + 3 * n_ep - 1) // (3 * n_ep)
    cap = (capacity + 15) // 16 * 16
    groups = 4
    rows = cap * (n_ep // groups)
    plan = gather_plan(n_tp)

    table_w = min(128, qw)
    operands = (
        queries, key_rows, values,
        query_gain.reshape(1, HEAD), key_gain.reshape(1, HEAD),
        mix_gain.reshape(n_tp, 1, qw),
        out_weight.reshape(n_tp, qw, out_w),
        expert_input,
        expert_gain.reshape(n_tp, 1, width),
        route_ids.T, route_weights.T,
        expert_gate.reshape(n_tp, width, ffw),
        expert_up.reshape(n_tp, width, ffw),
        expert_down.reshape(n_tp, ffw, out_w),
    )
    vmem = pl.BlockSpec(memory_space=pltpu.VMEM)
    hbm = pl.BlockSpec(memory_space=pl.ANY)
    specs = [hbm if i in (6, 11, 12, 13) else vmem for i in range(len(operands))]
    dma = pltpu.SemaphoreType.DMA
    line = n_ep == 4 and n_tp == 8
    tables_at = [pltpu.VMEM((length, table_w), F32)] * 2
    blocks_at = [
        pltpu.VMEM((n_ep, cap, width), BF16),
        pltpu.VMEM((groups, n_tp, rows, width), BF16),
        pltpu.VMEM((groups, n_tp, rows, ffw), BF16),
        pltpu.VMEM((n_tp, length, qw), BF16),
    ]
    weights_at = [
        pltpu.VMEM((n_tp, width, 2 * ffw), BF16),
        pltpu.VMEM((n_tp, ffw, out_w), BF16),
        pltpu.VMEM((n_tp, qw, out_w), BF16),
    ]
    results_at = [
        pltpu.VMEM((length, qw), BF16),
        pltpu.VMEM((groups, rows, out_w), BF16),
        pltpu.VMEM((n_ep, cap, out_w), BF16),
    ]
    if line:
        body = functools.partial(line_kernel, n_ep, n_tp, cap)
        scratch = tables_at + blocks_at + [pltpu.VMEM((n_ep, length, 2 * kw), BF16)]
        scratch += results_at + [pltpu.VMEM((2, length, out_w), F32)] + weights_at
        scratch += [dma((4,)), dma((3,)), dma((3, n_ep - 1)), dma((3,)), dma((2 * n_ep + 2, 4))]
    else:
        body = functools.partial(kernel, n_ep, n_tp, cap, plan)
        scratch = tables_at + blocks_at + [pltpu.VMEM((n_ep, length, kw), BF16)] * 2
        scratch += results_at + weights_at
        scratch += [dma((4, n_tp)), dma((1,))] + [dma((n_ep,))] * 8
        scratch += [dma((groups, len(plan)))] * 4 + [dma((len(plan),))] * 2
    outs = pl.pallas_call(
        body,
        out_shape=(
            pltpu.VMEM((length, out_w), BF16),
            pltpu.VMEM((length, out_w), BF16),
        ),
        in_specs=specs,
        out_specs=(vmem, vmem),
        scratch_shapes=scratch,
        compiler_params=pltpu.CompilerParams(
            collective_id=0, has_side_effects=True, vmem_limit_bytes=60 * 1024 * 1024
        ),
    )(*operands)
    return hand_out(outs)


def solution(mesh):
    placed = (
        P("ep", "tp"), P("ep", "tp"), P("ep", "tp"), P(), P(), P(), P(None, "tp"),
        P("ep", "tp"), P(), P("ep", None), P("ep", None),
        P("ep", None, "tp"), P("ep", None, "tp"), P("ep", None, "tp"),
    )
    return jax.shard_map(
        functools.partial(shards, mesh.shape["ep"], mesh.shape["tp"]),
        mesh=mesh,
        in_specs=placed,
        out_specs=(P("ep", "tp"), P("ep", "tp")),
        check_vma=False,
    )
```
